32 devices in a mesh: sp: 4 (over z), fs: 4 (over y, x), tp: 2 (over core).
Axes of the slice: x: 2, y: 2, z: 4, core: 2. Of those that a mesh axis runs over, the one named last changes fastest.
Arguments:
- tokens: bfloat16 [4, 1536, 2048], P('fs', ('sp', 'tp')), may hold values from -6 to 6
- norm_gain: float32 [2048], replicated, may hold values from 0.1 to 1.9
- conv_gate_w: bfloat16 [2048, 1024], P('sp', 'tp'), may hold values from -0.125 to 0.125
- conv_in_w: bfloat16 [2048, 1024], P('sp', 'tp'), may hold values from -0.125 to 0.125
- query_w: bfloat16 [2048, 1024], P('sp', 'tp'), may hold values from -0.125 to 0.125
- forget_w: bfloat16 [2048, 1024], P('sp', 'tp'), may hold values from -0.125 to 0.125
- value_w: bfloat16 [2048, 1024], P('sp', 'tp'), may hold values from -0.125 to 0.125
- conv_taps: float32 [3, 1024], P(None, 'tp'), may hold values from -3.5 to 3.5
- floor_gate: float32 [1024], P('tp'), may hold values from 0.93 to 1
- leak: float32 [4, 1536, 8], P('fs', 'sp', 'tp'), may hold values from -1.4 to 0
- head_gain: float32 [128], replicated, may hold values from 0.1 to 1.9
- conv_out_w: bfloat16 [1024, 2048], P('tp', 'fs'), may hold values from -0.125 to 0.125
- chain_out_w: bfloat16 [1024, 2048], P('tp', 'fs'), may hold values from -0.125 to 0.125
Outputs:
- mixed: bfloat16 [4, 1536, 2048], P('fs', ('sp', 'tp'))
The draws below stay inside these ranges and needn't reach their ends.
All inputs are finite; a program needn't handle non-finite values.
Results may differ from the reference program's by a relative error of at most 0.013.
Values may be sent and summed in bfloat16 or wider, within the bound.
A program may use at most 128 MiB of HBM per device.

```python
import jax
import jax.numpy as jnp
from jax import lax

D = 2048
CW = 1024
HEADS = 8
HEAD_DIM = 128
TOK = 384
BLOCK = 64
HW = 1024
SEQS = 4
LEN = 1536


def draw_floor_gate(key, part):
    base = jax.random.fold_in(key, 101)
    pick_key, fast_key, slow_key = jax.random.split(base, 3)
    fast_share = 0.5
    fast = jax.random.bernoulli(pick_key, fast_share, (HEADS, 1))
    fast_gap = jnp.exp(jax.random.uniform(fast_key, (HEADS, HEAD_DIM), jnp.float32, jnp.log(0.02), jnp.log(0.07)))
    slow_gap = jnp.exp(jax.random.uniform(slow_key, (HEADS, HEAD_DIM), jnp.float32, jnp.log(0.2), jnp.log(0.8))) / LEN
    return (1.0 - jnp.where(fast, fast_gap, slow_gap)).reshape(HEADS * HEAD_DIM).astype(jnp.float32)


def draw_leak(key, part):
    base = jax.random.fold_in(key, 202)
    rate_key, spot_key, depth_key = jax.random.split(base, 3)
    blocks = LEN // TOK
    rates = jnp.exp(jax.random.uniform(rate_key, (SEQS, blocks, 1, HEADS), jnp.float32, jnp.log(0.1), jnp.log(1.0))) / LEN
    constant_fading = -jnp.broadcast_to(rates, (SEQS, blocks, TOK, HEADS)).reshape(SEQS, LEN, HEADS)
    chosen_indices = jax.random.randint(spot_key, (SEQS, 1, HEADS, 2), 0, LEN)
    memory_width = jnp.log(jax.random.uniform(depth_key, (SEQS, 1, HEADS, 2), jnp.float32, 0.5, 0.8))
    sequence_slots = jnp.arange(LEN)[None, :, None, None]
    spike_clusters = jnp.sum(jnp.where(sequence_slots == chosen_indices, memory_width, 0.0), axis=3)
    return (constant_fading + spike_clusters).astype(jnp.float32)


def shard_levels(rng, dims, pieces, least, top_value):
    loudness = 1.0
    for position, parts in pieces:
        steps = jax.random.uniform(jax.random.fold_in(jax.random.fold_in(rng, 6), position), (parts,), jnp.float32, least / len(pieces), top_value / len(pieces))
        loudness = loudness * jnp.repeat(jnp.exp(steps), dims[position] // parts).reshape((-1,) + (1,) * (len(dims) - 1 - position))
    return loudness


def normal_values(stream_key, dims, scale, reach, cuts=(), dtype=jnp.bfloat16):
    values = jax.random.normal(stream_key, dims, jnp.float32) * scale
    if len(cuts) > 0:
        values = shard_levels(stream_key, dims, cuts, -0.22, 0.18) * values
    return jnp.clip(values, min=-reach, max=reach).astype(dtype)


def setup_inputs(seed: int = 0) -> dict:
    key_list = jax.random.split(jax.random.key(seed), 14)
    tokens = normal_values(key_list[0], (SEQS, LEN, D), 1.0, 6.0, ((0, 4), (1, 8)))
    norm_gain = jnp.clip(1.0 + 0.18 * jax.random.normal(key_list[1], (D,), jnp.float32), 0.1, 1.9)
    conv_gate_w = normal_values(key_list[2], (D, CW), D ** -0.5, 0.125, ((0, 4), (1, 2)))
    conv_in_w = normal_values(key_list[3], (D, CW), D ** -0.5, 0.125, ((0, 4), (1, 2)))
    query_w = normal_values(key_list[4], (D, HW), D ** -0.5, 0.125, ((0, 4), (1, 2)))
    forget_w = normal_values(key_list[5], (D, HW), D ** -0.5, 0.125, ((0, 4), (1, 2)))
    value_w = normal_values(key_list[6], (D, HW), D ** -0.5, 0.125, ((0, 4), (1, 2)))
    conv_taps = normal_values(key_list[7], (3, CW), 3 ** -0.5, 3.5, ((1, 2),), jnp.float32)
    floor_gate = draw_floor_gate(jax.random.fold_in(key_list[13], 71), 0)
    leak = draw_leak(jax.random.fold_in(key_list[13], 71), 0)
    head_gain = jnp.clip(1.0 + 0.18 * jax.random.normal(key_list[10], (HEAD_DIM,), jnp.float32), 0.1, 1.9)
    conv_out_w = normal_values(key_list[11], (CW, D), (CW + HW) ** -0.5, 0.125, ((0, 2), (1, 4)))
    chain_out_w = normal_values(key_list[12], (HW, D), (CW + HW) ** -0.5, 0.125, ((0, 2), (1, 4)))
    return {"tokens": tokens, "norm_gain": norm_gain, "conv_gate_w": conv_gate_w, "conv_in_w": conv_in_w, "query_w": query_w, "forget_w": forget_w, "value_w": value_w, "conv_taps": conv_taps, "floor_gate": floor_gate, "leak": leak, "head_gain": head_gain, "conv_out_w": conv_out_w, "chain_out_w": chain_out_w}


HIGH_ACCURACY = lax.Precision.HIGHEST

def norm_rows(matrix, norm_gain):
    values = matrix.astype(jnp.float32)
    center = values - lax.optimization_barrier(jnp.mean(values, axis=-1, keepdims=True))
    spread = lax.optimization_barrier(jnp.mean(center * center, axis=-1, keepdims=True))
    return (center * lax.rsqrt(spread + 1e-05) * norm_gain).astype(jnp.bfloat16)

def block_chain(query, keys, values, decay):
    heads, length, width = query.shape
    count = length // BLOCK

    def split_blocks(array):
        return array.reshape(heads, count, BLOCK, array.shape[-1]).transpose(1, 0, 2, 3)
    causal = jnp.tril(jnp.ones((BLOCK, BLOCK), jnp.float32))

    def advance(hidden_state, inputs):
        query_part, key_portion, value_portion, decay_part = inputs
        running_state = jnp.cumsum(decay_part, axis=1)
        scaled_query = query_part * jnp.exp(running_state)
        key_scaled = key_portion * jnp.exp(-running_state)
        scores = jnp.einsum('htk,hsk->hts', scaled_query, key_scaled, precision=HIGH_ACCURACY) * causal
        inside = jnp.einsum('hts,hsv->htv', scores, value_portion, precision=HIGH_ACCURACY)
        carried_state = jnp.einsum('rgn,rns->rgs', scaled_query, hidden_state, precision=HIGH_ACCURACY)
        final_state = running_state[:, -1:, :]
        state_update = jnp.einsum('qdm,qdt->qmt', key_portion * jnp.exp(final_state - running_state), value_portion, precision=HIGH_ACCURACY)
        return (jnp.exp(final_state[:, 0, :])[:, :, None] * hidden_state + state_update, inside + carried_state)
    initial = jnp.zeros((heads, width, values.shape[-1]), jnp.float32)
    hidden_state, layer_results = lax.scan(advance, initial, (split_blocks(query), split_blocks(keys), split_blocks(values), split_blocks(decay)))
    return (layer_results.transpose(1, 0, 2, 3).reshape(heads, length, values.shape[-1]), hidden_state)

def reference(tokens, norm_gain, conv_gate_w, conv_in_w, query_w, forget_w, value_w, conv_taps, floor_gate, leak, head_gain, conv_out_w, chain_out_w):
    seqs, length, width = tokens.shape
    normed = norm_rows(tokens.reshape(seqs * length, width), norm_gain)

    def project(weight):
        product = jnp.dot(normed, weight, preferred_element_type=jnp.float32)
        return product.astype(jnp.bfloat16).reshape(seqs, length, weight.shape[1])
    second_gate = project(conv_gate_w)
    signal = project(conv_in_w)
    query_raw = project(query_w)
    forget_raw = project(forget_w)
    value_raw = project(value_w)
    margin = conv_taps.shape[0] - 1
    padded = jnp.pad(signal.astype(jnp.float32), ((0, 0), (margin, 0), (0, 0)))
    filtered = jnp.zeros((seqs, length, signal.shape[2]), jnp.float32)
    for offset in range(margin + 1):
        filtered = filtered + conv_taps[offset] * padded[:, offset:offset + length]
    conv_mix = (second_gate.astype(jnp.float32) * filtered).astype(jnp.bfloat16)

    def chain_sequence(inputs):
        query_rows, forget_rows, value_rows, leak_rows = inputs

        def by_head(array):
            return array.astype(jnp.float32).reshape(length, HEADS, HEAD_DIM).transpose(1, 0, 2)
        floor = floor_gate.reshape(HEADS, 1, HEAD_DIM)
        logits = by_head(forget_rows)
        retain = floor + (1.0 - floor) * jax.nn.sigmoid(logits)
        keys = (1.0 - floor) * jax.nn.sigmoid(-logits)
        decay = jnp.log(retain) + leak_rows.T[:, :, None]
        layer_results, _ = block_chain(jax.nn.silu(by_head(query_rows)), keys, by_head(value_rows), decay)
        scale = lax.rsqrt(lax.optimization_barrier(jnp.mean(layer_results * layer_results, axis=-1, keepdims=True)) + 1e-06)
        normal_out = layer_results * scale * head_gain
        return normal_out.transpose(1, 0, 2).reshape(length, HEADS * HEAD_DIM).astype(jnp.bfloat16)
    chain_mix = lax.map(chain_sequence, (query_raw, forget_raw, value_raw, leak))
    mixed = jnp.dot(conv_mix.reshape(seqs * length, -1), conv_out_w, preferred_element_type=jnp.float32)
    mixed = mixed + jnp.dot(chain_mix.reshape(seqs * length, -1), chain_out_w, preferred_element_type=jnp.float32)
    return mixed.astype(jnp.bfloat16).reshape(seqs, length, width)
```

```python
import functools

import jax
import jax.numpy as jnp
from jax import lax
from jax.experimental import pallas as pl
from jax.experimental.pallas import tpu as pltpu
from jax.sharding import PartitionSpec as P

MESH = pl.DeviceIdType.MESH
BF = jnp.bfloat16
F32 = jnp.float32
NT = (((1,), (1,)), ((), ()))
TN = (((0,), (0,)), ((), ()))
GATE, SIGNAL, QUERY, FORGET, VALUE = 4, 3, 1, 0, 2


def kernel(
    ns, nf,
    tok, gain, w0, w1, w2, w3, w4, taps, floor, leak_t, hgain, cow, how,
    out,
    tokv, rows, wg, y, wo, rim, inside, reach, states, sdecay, sin, sout,
    lk, lcol, lrow, msend, mix, osend, orecv, mine,
    tl, zs, zsl, zr, zloc, rs, rr, ts, tr, ls, lr, oloc, os_, or_, rl, za, xs, xr, ms, mr, ss, sr, es, er,
):
    s, f, t = lax.axis_index("sp"), lax.axis_index("fs"), lax.axis_index("tp")
    other = 1 - t
    half = tok.shape[1]
    length = 2 * half
    kd = w0.shape[0]
    wide = w0.shape[1] // nf
    ws = (w3, w2, w4, w1, w0)
    np_ = len(ws)
    has_left, has_right = s > 0, s < ns - 1
    outs = (cow, how)
    cols = wo.shape[3]
    odd = lax.rem(s, 2)
    mate = s + 1 - 2 * odd

    def remote(src, dst, send, recv, **where):
        return pltpu.make_async_remote_copy(
            src_ref=src, dst_ref=dst, send_sem=send, recv_sem=recv,
            device_id=where, device_id_type=MESH,
        )

    def wblock(b, p):
        return wg.at[p, pl.ds(pl.multiple_of(b * kd, kd), kd), :]

    def wload(p):
        return pltpu.make_async_copy(
            ws[p].at[:, pl.ds(pl.multiple_of(f * wide, wide), wide)], wblock(s, p), zloc.at[p]
        )

    def oload(j):
        return pltpu.make_async_copy(outs[j], wo.at[f, j], oloc.at[j])

    tload = pltpu.make_async_copy(tok.at[0], tokv, tl.at[0])
    wload(0).start()
    tload.start()
    for p in range(1, np_):
        wload(p).start()
    for j in range(2):
        oload(j).start()

    barrier = pltpu.get_barrier_semaphore()
    pl.semaphore_signal(barrier, inc=1, device_id={"tp": other}, device_id_type=MESH)
    for d in range(1, nf):
        pl.semaphore_signal(barrier, inc=1, device_id={"fs": f ^ d}, device_id_type=MESH)

    @pl.when(has_left)
    def _():
        pl.semaphore_signal(barrier, inc=1, device_id={"sp": s - 1}, device_id_type=MESH)

    @pl.when(has_right)
    def _():
        pl.semaphore_signal(barrier, inc=1, device_id={"sp": s + 1}, device_id_type=MESH)

    heads = leak_t.shape[0]
    lk[f, pl.ds(0, heads), :] = leak_t[...]
    ends = jnp.where(has_left, 1, 0) + jnp.where(has_right, 1, 0)
    pl.semaphore_wait(barrier, nf + ends)


    def own_right(p):
        return remote(wblock(s, p), wblock(s, p), zs.at[s, p], zr.at[s, p], sp=s + 1)

    def own_left(p):
        return remote(wblock(s, p), wblock(s, p), zsl.at[p], zr.at[s, p], sp=s - 1)

    def relay(b, p, to):
        return remote(wblock(b, p), wblock(b, p), zs.at[b, p], zr.at[b, p], sp=to)

    def send_own(p):
        wload(p).wait()

        @pl.when(has_right)
        def _():
            own_right(p).start()

        @pl.when(has_left)
        def _():
            own_left(p).start()

    def zhop(k, p):
        @pl.when((s - k >= 0) & has_right)
        def _():
            relay(s - k, p, s + 1).wait_recv()
            relay(s - k, p, s + 1).start()

        @pl.when((s + k < ns) & has_left)
        def _():
            relay(s + k, p, s - 1).wait_recv()
            relay(s + k, p, s - 1).start()

    def zfar(p):
        def hop(k, carry):
            zhop(k, p)
            return carry

        if ns > 3:
            lax.fori_loop(3, ns, hop, 0)

    def zready(p):
        def hop(k, carry):
            @pl.when((s - k >= 0) & (s == ns - 1))
            def _():
                relay(s - k, p, s - 1).wait_recv()

            @pl.when((s + k < ns) & (s == 0))
            def _():
                relay(s + k, p, s + 1).wait_recv()

            return carry

        lax.fori_loop(1, ns, hop, 0)

    send_own(0)
    send_own(1)


    tload.wait()
    x = tokv[...].astype(F32)
    center = x - jnp.mean(x, axis=-1, keepdims=True)
    spread = jnp.mean(center * center, axis=-1, keepdims=True)
    rows[f, pl.ds(pl.multiple_of(t * half, half), half), :] = (
        center * lax.rsqrt(spread + 1e-05) * gain[...]
    ).astype(BF)

    quarter = half // 2

    def piece(g, j):
        return rows.at[g, pl.ds(pl.multiple_of(t * half + j * quarter, quarter), quarter), :]

    def core_rows(g, core):
        return rows.at[g, pl.ds(pl.multiple_of(core * half, half), half), :]

    def row_arrived(d, j):
        g = f ^ d
        remote(piece(g, j), piece(g, j), rs.at[0], rr.at[d, j], fs=f ^ 1).wait_recv()

    def row_send(d, j, to_d, slot):
        g = f ^ d
        to = f ^ to_d
        return remote(piece(g, j), piece(g, j), rs.at[slot], rr.at[d ^ to_d, j], fs=to)

    def twin(d):
        g = f ^ d
        return remote(core_rows(g, t), core_rows(g, t), ts.at[d], tr.at[d], tp=other)

    def twin_arrived(d):
        g = f ^ d
        remote(core_rows(g, other), core_rows(g, other), ts.at[d], tr.at[d], tp=other).wait_recv()

    def leak_send(d):
        return remote(lk.at[f], lk.at[f], ls.at[d], lr.at[d], fs=f ^ d)

    def leak_arrived(d):
        g = f ^ d
        remote(lk.at[g], lk.at[g], ls.at[d], lr.at[d], fs=g).wait_recv()

    for d in range(1, nf):
        leak_send(d).start()
    row_send(0, 0, 1, 0).start()
    row_send(0, 1, 2, 1).start()
    row_send(0, 1, 1, 2).start()
    row_send(0, 0, 2, 3).start()
    twin(0).start()

    zhop(1, 0)
    zhop(1, 1)
    zhop(2, 0)
    send_own(2)


    for d in range(1, nf):
        leak_arrived(d)
    ri = lax.broadcasted_iota(jnp.int32, (length, length), 0)
    ci = lax.broadcasted_iota(jnp.int32, (length, length), 1)
    tril = (ri >= ci).astype(F32)
    triu = (ri <= ci).astype(F32)
    high = lax.Precision.HIGHEST
    mine_leak = jnp.concatenate(
        [lk[g, pl.ds(f, 1), :] for g in range(nf)] + [jnp.zeros((8 - nf, length), F32)], axis=0
    )
    lsum = lax.dot_general(tril, mine_leak, NT, precision=high, preferred_element_type=F32)
    lsum_t = jnp.dot(mine_leak, triu, precision=high, preferred_element_type=F32)
    for g in range(nf):
        lcol[g] = jnp.broadcast_to(lsum[:, g : g + 1], (length, wide))
        lrow[g] = jnp.broadcast_to(lsum_t[g : g + 1, :], (8, length))


    pw = cols // 4

    def opiece(g, q):
        return wo.at[g, :, :, pl.ds(pl.multiple_of(q * pw, pw), pw)]

    def order(to_d, i):
        first = 2 * odd + (1 if to_d == 1 else 0)
        second = 2 * odd + (0 if to_d == 1 else 1)
        return (first, second, 2 - 2 * odd, 3 - 2 * odd)[i]

    def own_out(to_d, i):
        q = order(to_d, i)
        return remote(opiece(f, q), opiece(f, q), os_.at[to_d, i], or_.at[to_d, q], fs=f ^ to_d)

    def out_arrived(d, q):
        g = f ^ d
        remote(opiece(g, q), opiece(g, q), os_.at[1, 0], or_.at[d, q], fs=f ^ 1).wait_recv()

    def relay_out(d, to_d):
        g = f ^ d
        q = order(d, 0)
        return remote(opiece(g, q), opiece(g, q), rl.at[to_d], or_.at[3, q], fs=f ^ to_d)

    def assist(i):
        g = f ^ 3
        q = 2 * odd + i
        return remote(opiece(g, q), opiece(g, q), za.at[i], or_.at[3, q], sp=mate)

    row_arrived(1, 0)
    row_send(1, 0, 2, 4).start()
    row_arrived(2, 1)
    row_send(2, 1, 1, 5).start()
    for j in range(2):
        oload(j).wait()
    for i in range(2):
        own_out(1, i).start()
        own_out(2, i).start()

    zhop(1, 2)
    zhop(2, 1)
    zfar(0)
    zready(0)

    def project(d, p):
        g = f ^ d
        y[g, p] = jnp.dot(rows[g], wg[p], preferred_element_type=F32).astype(BF)

    twin_arrived(0)
    project(0, 0)
    zhop(2, 2)
    send_own(3)
    row_arrived(1, 1)
    twin(1).start()
    row_arrived(2, 0)
    twin(2).start()
    zhop(1, 3)
    send_own(4)
    zfar(1)
    zready(1)
    project(0, 1)
    zhop(1, 4)
    zfar(2)
    zready(2)
    project(0, 2)
    zhop(2, 3)

    causal = ri >= ci
    tril_short = tril.astype(BF)

    def local(d):
        g = f ^ d
        fl = floor[f]
        logits = y[g, FORGET].astype(F32)
        retain = fl + (1.0 - fl) * jax.nn.sigmoid(logits)
        keys = (1.0 - fl) * jax.nn.sigmoid(-logits)
        step = jnp.log(retain)
        coarse = step.astype(BF)
        fine = (step - coarse.astype(F32)).astype(BF)
        both = jnp.dot(
            tril_short, jnp.concatenate([coarse, fine], axis=1), preferred_element_type=F32
        )
        total = both[:, :wide] + both[:, wide:]
        raw = y[g, QUERY].astype(F32)
        query = raw * jax.nn.sigmoid(raw) * jnp.exp(total)
        value = y[g, VALUE]
        scores = lax.dot_general(
            query.astype(BF), (keys * jnp.exp(-total)).astype(BF), NT, preferred_element_type=F32
        )
        lc = lcol[g]
        gap = lc[:, 0:1] - lrow[g, 0:1, :]
        scores = jnp.where(causal, scores * jnp.exp(jnp.where(causal, gap, 0.0)), 0.0)
        inside[g] = jnp.dot(scores.astype(BF), value, preferred_element_type=F32)
        reach[g] = (query * jnp.exp(lc)).astype(BF)
        full = total + lc
        end = full[length - 1 :, :]
        update = (keys * jnp.exp(end - full)).astype(BF)
        states[g] = lax.dot_general(value, update, TN, preferred_element_type=F32)
        sdecay[g] = jnp.broadcast_to(jnp.exp(end), (8, wide))

    def many(body, first, last):
        def one(d, carry):
            body(d)
            return carry

        lax.fori_loop(first, last, one, 0)

    def project_chain(d):
        for p in range(3):
            project(d, p)

    row_arrived(3, 0)
    row_arrived(3, 1)
    twin(3).start()
    local(0)
    zhop(2, 4)
    twin_arrived(1)
    twin_arrived(2)

    def both_steps(d):
        project_chain(d)
        local(d)

    many(both_steps, 1, 3)
    twin_arrived(3)
    many(both_steps, 3, 4)

    out_arrived(2, order(2, 0))
    relay_out(2, 1).start()
    out_arrived(1, order(1, 0))
    relay_out(1, 2).start()
    own_out(1, 2).start()
    own_out(2, 2).start()

    def state_copy(g):
        return remote(sout.at[g], sin.at[g], ss.at[g], sr.at[g], sp=s + 1)

    def place(j, g):
        return mix.at[j, :, pl.ds(pl.multiple_of(g * wide, wide), wide)]

    def mixed_send(d, j):
        return remote(msend.at[d, j], place(j, f), xs.at[d, j], xr.at[d, j], fs=f ^ d)

    def mixed_arrived(d, j):
        remote(msend.at[d, j], place(j, f ^ d), xs.at[d, j], xr.at[d, j], fs=f ^ d).wait_recv()

    def deliver(d, j, value):
        @pl.when(d == 0)
        def _():
            mix[j, :, pl.ds(pl.multiple_of(f * wide, wide), wide)] = value

        @pl.when(d > 0)
        def _():
            msend[d, j] = value
            mixed_send(d, j).start()

    def chain(d):
        g = f ^ d

        @pl.when(has_left)
        def _():
            state_copy(g).wait_recv()

        @pl.when(s == 0)
        def _():
            sin[g] = jnp.zeros(sin.shape[1:], BF)

        @pl.when(has_right)
        def _():
            sout[g] = (sin[g].astype(F32) * sdecay[g, 0:1, :] + states[g]).astype(BF)
            state_copy(g).start()

        raw = inside[g] + lax.dot_general(reach[g], sin[g], NT, preferred_element_type=F32)
        scale = lax.rsqrt(jnp.mean(raw * raw, axis=-1, keepdims=True) + 1e-06)
        deliver(d, 1, (raw * scale * hgain[...]).astype(BF))

    many(chain, 0, nf)


    edge = rim.shape[1]

    def rim_copy(g):
        return remote(
            y.at[g, SIGNAL, pl.ds(length - edge, edge), :], rim.at[g],
            ms.at[g], mr.at[g], sp=s + 1,
        )

    zfar(3)
    zready(3)

    def signal(d):
        g = f ^ d
        project(d, 3)

        @pl.when(has_right)
        def _():
            rim_copy(g).start()

        @pl.when(s == 0)
        def _():
            rim[g] = jnp.zeros((edge, wide), BF)

    many(signal, 0, nf)
    zfar(4)
    zready(4)

    def conv(d):
        g = f ^ d
        project(d, 4)

        @pl.when(has_left)
        def _():
            rim_copy(g).wait_recv()

        padded = jnp.concatenate([rim[g], y[g, SIGNAL]], axis=0).astype(F32)
        margin = taps.shape[1] - 1
        filtered = jnp.zeros((length, wide), F32)
        for o in range(margin + 1):
            start = edge - margin + o
            filtered = filtered + taps[f, o : o + 1, :] * padded[start : start + length]
        deliver(d, 0, (y[g, GATE].astype(F32) * filtered).astype(BF))

    many(conv, 0, nf)
    own_out(1, 3).start()
    own_out(2, 3).start()
    for i in range(2):
        out_arrived(3, 2 * odd + i)
        assist(i).start()


    def share(i):
        return remote(osend.at[i], orecv.at[i], es.at[i], er.at[i], tp=other)

    for d in range(1, nf):
        for j in range(2):
            mixed_arrived(d, j)

    def partial(g, c, who):
        at = pl.ds(pl.multiple_of(who * half, half), half)
        co = pl.ds(pl.multiple_of(c * 2 * pw, 2 * pw), 2 * pw)
        return jnp.dot(mix[0, at, :], wo[g, 0, :, co], preferred_element_type=F32) + jnp.dot(
            mix[1, at, :], wo[g, 1, :, co], preferred_element_type=F32
        )

    def begin(i, d, c):
        g = f ^ d
        osend[i] = partial(g, c, other)
        share(i).start()
        mine[i] = partial(g, c, t)

    def finish(i, d, c):
        g = f ^ d
        share(i).wait_recv()
        at = pl.ds(pl.multiple_of(g * cols + c * 2 * pw, 2 * pw), 2 * pw)
        out[0, :, at] = (mine[i] + orecv[i]).astype(BF)

    plan = [
        (0, odd, ()),
        (0, 1 - odd, ()),
        (1, odd, (order(1, 1),)),
        (2, odd, (order(2, 1),)),
        (3, odd, ()),
        (3, 1 - odd, (2 - 2 * odd, 3 - 2 * odd)),
        (1, 1 - odd, (2 - 2 * odd, 3 - 2 * odd)),
        (2, 1 - odd, (2 - 2 * odd, 3 - 2 * odd)),
    ]
    for i, (d, c, waits) in enumerate(plan):
        for q in waits:
            out_arrived(d, q)
        begin(i, d, c)
        if i:
            finish(i - 1, *plan[i - 1][:2])
    finish(len(plan) - 1, *plan[-1][:2])


    for p in range(np_):
        def drained(b, carry, p=p):
            @pl.when(((b < s) & has_right) | ((b > s) & has_left))
            def _():
                relay(b, p, s).wait_send()

            return carry

        lax.fori_loop(0, ns, drained, 0)

        @pl.when(has_right)
        def _(p=p):
            own_right(p).wait_send()

        @pl.when(has_left)
        def _(p=p):
            own_left(p).wait_send()

    for d, j, to_d, slot in ((0, 0, 1, 0), (0, 1, 2, 1), (0, 1, 1, 2), (0, 0, 2, 3), (1, 0, 2, 4), (2, 1, 1, 5)):
        row_send(d, j, to_d, slot).wait_send()
    for to_d in range(1, 3):
        for i in range(4):
            own_out(to_d, i).wait_send()
        relay_out(3 - to_d, to_d).wait_send()
    for i in range(2):
        assist(i).wait_send()
    for d in range(nf):
        twin(d).wait_send()
        if d:
            leak_send(d).wait_send()
            for j in range(2):
                mixed_send(d, j).wait_send()
    for i in range(len(plan)):
        share(i).wait_send()

    @pl.when(has_right)
    def _():
        for g in range(nf):
            state_copy(g).wait_send()
            rim_copy(g).wait_send()


def body(ns, nf, tokens, norm_gain, w0, w1, w2, w3, w4, conv_taps, floor_gate, leak, head_gain, cow, how):
    half, width = tokens.shape[1:]
    length = 2 * half
    heads = leak.shape[2]
    kd = w0.shape[0]
    wide = w0.shape[1] // nf
    assert heads == nf and nf == 4 and floor_gate.shape[0] == heads * wide and ns % 2 == 0
    taps = conv_taps.reshape(conv_taps.shape[0], nf, wide).transpose(1, 0, 2)
    vm = pl.BlockSpec(memory_space=pltpu.VMEM)
    hbm = pl.BlockSpec(memory_space=pl.ANY)
    dma = pltpu.SemaphoreType.DMA
    cols = cow.shape[1]
    scratch = [
        pltpu.VMEM((half, width), BF),
        pltpu.VMEM((nf, length, width), BF),
        pltpu.VMEM((5, ns * kd, wide), BF),
        pltpu.VMEM((nf, 5, length, wide), BF),
        pltpu.VMEM((nf, 2) + cow.shape, BF),
        pltpu.VMEM((nf, 16, wide), BF),
        pltpu.VMEM((nf, length, wide), F32),
        pltpu.VMEM((nf, length, wide), BF),
        pltpu.VMEM((nf, wide, wide), F32),
        pltpu.VMEM((nf, 8, wide), F32),
        pltpu.VMEM((nf, wide, wide), BF),
        pltpu.VMEM((nf, wide, wide), BF),
        pltpu.VMEM((nf, 8, length), F32),
        pltpu.VMEM((nf, length, wide), F32),
        pltpu.VMEM((nf, 8, length), F32),
        pltpu.VMEM((nf, 2, length, wide), BF),
        pltpu.VMEM((2, length, nf * wide), BF),
        pltpu.VMEM((2 * nf, half, cols // 2), F32),
        pltpu.VMEM((2 * nf, half, cols // 2), F32),
        pltpu.VMEM((2 * nf, half, cols // 2), F32),
        dma((1,)), dma((ns, 5)), dma((5,)), dma((ns, 5)), dma((5,)),
        dma((6,)), dma((nf, 2)), dma((nf,)), dma((nf,)), dma((nf,)), dma((nf,)),
        dma((2,)), dma((3, 4)), dma((nf, 4)), dma((3,)), dma((2,)),
        dma((nf, 2)), dma((nf, 2)), dma((nf,)), dma((nf,)), dma((nf,)), dma((nf,)),
        dma((2 * nf,)), dma((2 * nf,)),
    ]
    return pl.pallas_call(
        functools.partial(kernel, ns, nf),
        out_shape=jax.ShapeDtypeStruct(tokens.shape, BF),
        in_specs=[hbm, vm, hbm, hbm, hbm, hbm, hbm, vm, vm, vm, vm, hbm, hbm],
        out_specs=vm,
        scratch_shapes=scratch,
        compiler_params=pltpu.CompilerParams(
            collective_id=0, has_side_effects=True, vmem_limit_bytes=48 * 2**20
        ),
    )(
        tokens, norm_gain[None], w0, w1, w2, w3, w4, taps, floor_gate.reshape(heads, 1, wide),
        leak[0].T, head_gain[None], cow, how,
    )


def solution(mesh):
    in_specs = (
        P("fs", ("sp", "tp"), None),
        P(),
        P("sp", "tp"),
        P("sp", "tp"),
        P("sp", "tp"),
        P("sp", "tp"),
        P("sp", "tp"),
        P(None, "tp"),
        P("tp"),
        P("fs", "sp", "tp"),
        P(),
        P("tp", "fs"),
        P("tp", "fs"),
    )
    out_specs = P("fs", ("sp", "tp"), None)
    step = functools.partial(body, mesh.shape["sp"], mesh.shape["fs"])
    return jax.shard_map(step, mesh=mesh, in_specs=in_specs, out_specs=out_specs, check_vma=False)
```

```python
import functools

import jax
import jax.numpy as jnp
from jax import lax
from jax.experimental import pallas as pl
from jax.experimental.pallas import tpu as pltpu
from jax.sharding import PartitionSpec as P

MESH = pl.DeviceIdType.MESH
BF = jnp.bfloat16
F32 = jnp.float32
NT = (((1,), (1,)), ((), ()))
TN = (((0,), (0,)), ((), ()))
GATE, SIGNAL, QUERY, FORGET, VALUE = 4, 3, 1, 0, 2


def kernel(
    ns, nf,
    tok_h, gain_h, w0, w1, w2, w3, w4, taps_h, floor_h, leak_h, hgain_h, cow, how,
    out,
    tokv, gain, taps, floor, leak_t, hgain,
    rows, wg, y, wo, rim, filt, inside, reach, states, sdecay, sin, sout,
    lk, lcol, lrow, msend, mix, acc, orecv,
    il, zs, zsl, zr, zloc, rs, rr, ts, tr, ls, lr, oloc, os_, or_, rl, za, xs, xr, ms, mr, ss, sr, es, er,
):
    s, f, t = lax.axis_index("sp"), lax.axis_index("fs"), lax.axis_index("tp")
    other = 1 - t
    half = tokv.shape[0]
    length = 2 * half
    kd = w0.shape[0]
    wide = w0.shape[1] // nf
    ws = (w3, w2, w4, w1, w0)
    np_ = len(ws)
    has_left, has_right = s > 0, s < ns - 1
    inner = has_left & has_right
    outs = (cow, how)
    depth, cols = cow.shape
    odd = lax.rem(s, 2)
    mate = s + 1 - 2 * odd

    def remote(src, dst, send, recv, **where):
        return pltpu.make_async_remote_copy(
            src_ref=src, dst_ref=dst, send_sem=send, recv_sem=recv,
            device_id=where, device_id_type=MESH,
        )


    def wblock(b, p):
        return wg.at[pl.ds(pl.multiple_of(b * kd, kd), kd), pl.ds(p * wide, wide)]

    def wload(p):
        return pltpu.make_async_copy(
            ws[p].at[:, pl.ds(pl.multiple_of(f * wide, wide), wide)], wblock(s, p), zloc.at[p]
        )

    def oload(j):
        return pltpu.make_async_copy(outs[j], wo.at[0, pl.ds(j * depth, depth), :], oloc.at[j])

    loads = [
        pltpu.make_async_copy(src, dst, il.at[i])
        for i, (src, dst) in enumerate(
            ((tok_h.at[0], tokv), (gain_h, gain), (leak_h, leak_t), (taps_h, taps), (floor_h, floor), (hgain_h, hgain))
        )
    ]

    wload(0).start()
    loads[0].start()
    wload(1).start()
    for load in loads[1:]:
        load.start()
    for p in range(2, np_):
        wload(p).start()
    for j in range(2):
        oload(j).start()

    barrier = pltpu.get_barrier_semaphore()
    for d in range(nf - 1, 0, -1):
        pl.semaphore_signal(barrier, inc=1, device_id={"fs": f ^ d}, device_id_type=MESH)

    @pl.when(has_left)
    def _():
        pl.semaphore_signal(barrier, inc=1, device_id={"sp": s - 1}, device_id_type=MESH)

    @pl.when(has_right)
    def _():
        pl.semaphore_signal(barrier, inc=1, device_id={"sp": s + 1}, device_id_type=MESH)

    pl.semaphore_signal(barrier, inc=1, device_id={"tp": other}, device_id_type=MESH)


    for load in loads[:3]:
        load.wait()
    lk[0, pl.ds(0, leak_t.shape[0]), :] = leak_t[...]
    x = tokv[...].astype(F32)
    center = x - jnp.mean(x, axis=-1, keepdims=True)
    spread = jnp.mean(center * center, axis=-1, keepdims=True)
    rows[0, pl.ds(pl.multiple_of(t * half, half), half), :] = (
        center * lax.rsqrt(spread + 1e-05) * gain[...]
    ).astype(BF)

    ends = jnp.where(has_left, 1, 0) + jnp.where(has_right, 1, 0)
    pl.semaphore_wait(barrier, nf + ends)


    def own_right(p):
        return remote(wblock(s, p), wblock(s, p), zs.at[s, p], zr.at[s, p], sp=s + 1)

    def own_left(p):
        return remote(wblock(s, p), wblock(s, p), zsl.at[p], zr.at[s, p], sp=s - 1)

    def relay(b, p, to):
        return remote(wblock(b, p), wblock(b, p), zs.at[b, p], zr.at[b, p], sp=to)

    def send_own(p, where):
        @pl.when(where & has_right)
        def _():
            own_right(p).start()

        @pl.when(where & has_left)
        def _():
            own_left(p).start()

    def zhop(k, p):
        @pl.when((s - k >= 0) & has_right)
        def _():
            relay(s - k, p, s + 1).wait_recv()
            relay(s - k, p, s + 1).start()

        @pl.when((s + k < ns) & has_left)
        def _():
            relay(s + k, p, s - 1).wait_recv()
            relay(s + k, p, s - 1).start()

    def zready(p):
        def far(k, carry):
            zhop(k, p)
            return carry

        if ns > 3:
            lax.fori_loop(3, ns, far, 0)

        def hop(k, carry):
            @pl.when((s - k >= 0) & (s == ns - 1))
            def _():
                relay(s - k, p, s - 1).wait_recv()

            @pl.when((s + k < ns) & (s == 0))
            def _():
                relay(s + k, p, s + 1).wait_recv()

            return carry

        lax.fori_loop(1, ns, hop, 0)

    always = s >= 0
    for p in range(2):
        wload(p).wait()
        send_own(p, always)

    quarter = half // 2

    def piece(d, j):
        return rows.at[d, pl.ds(pl.multiple_of(t * half + j * quarter, quarter), quarter), :]

    def core_rows(d, core):
        return rows.at[d, pl.ds(pl.multiple_of(core * half, half), half), :]

    def row_send(d, j, to_d, slot):
        return remote(piece(d, j), piece(d ^ to_d, j), rs.at[slot], rr.at[d ^ to_d, j], fs=f ^ to_d)

    def row_arrived(d, j):
        remote(piece(d, j), piece(d, j), rs.at[0], rr.at[d, j], fs=f ^ 1).wait_recv()

    def twin(d):
        return remote(core_rows(d, t), core_rows(d, t), ts.at[d], tr.at[d], tp=other)

    def twin_arrived(d):
        remote(core_rows(d, other), core_rows(d, other), ts.at[d], tr.at[d], tp=other).wait_recv()

    def leak_send(d):
        return remote(lk.at[0], lk.at[d], ls.at[d], lr.at[d], fs=f ^ d)

    def leak_arrived(d):
        remote(lk.at[d], lk.at[d], ls.at[d], lr.at[d], fs=f ^ 1).wait_recv()

    for d in range(1, nf):
        leak_send(d).start()
    row_send(0, 0, 1, 0).start()
    row_send(0, 1, 2, 1).start()
    row_send(0, 1, 1, 2).start()
    row_send(0, 0, 2, 3).start()
    twin(0).start()
    for p in range(2, np_):
        wload(p).wait()
        send_own(p, jnp.logical_not(inner))

    zhop(1, 0)
    zhop(1, 1)


    for d in range(1, nf):
        leak_arrived(d)
    ri = lax.broadcasted_iota(jnp.int32, (length, length), 0)
    ci = lax.broadcasted_iota(jnp.int32, (length, length), 1)
    tril = (ri >= ci).astype(F32)
    triu = (ri <= ci).astype(F32)
    high = lax.Precision.HIGHEST
    head_leak = jnp.concatenate(
        [lk[d, pl.ds(f, 1), :] for d in range(nf)] + [jnp.zeros((8 - nf, length), F32)], axis=0
    )
    lsum = lax.dot_general(tril, head_leak, NT, precision=high, preferred_element_type=F32)
    lsum_t = jnp.dot(head_leak, triu, precision=high, preferred_element_type=F32)
    for d in range(nf):
        lcol[d] = jnp.broadcast_to(lsum[:, d : d + 1], (length, wide))
        lrow[d] = jnp.broadcast_to(lsum_t[d : d + 1, :], (8, length))

    zhop(2, 0)
    send_own(2, inner)


    pw = cols // 4

    def opiece(d, q):
        return wo.at[d, :, pl.ds(pl.multiple_of(q * pw, pw), pw)]

    def order(to_d, i):
        first = 2 * odd + (1 if to_d == 1 else 0)
        second = 2 * odd + (0 if to_d == 1 else 1)
        return (first, second, 2 - 2 * odd, 3 - 2 * odd)[i]

    def own_out(to_d, i):
        q = order(to_d, i)
        return remote(opiece(0, q), opiece(to_d, q), os_.at[to_d, i], or_.at[to_d, q], fs=f ^ to_d)

    def out_arrived(d, q):
        remote(opiece(d, q), opiece(d, q), os_.at[1, 0], or_.at[d, q], fs=f ^ 1).wait_recv()

    def relay_out(d, to_d):
        q = order(d, 0)
        return remote(opiece(d, q), opiece(3, q), rl.at[to_d], or_.at[3, q], fs=f ^ to_d)

    def assist(i):
        q = 2 * odd + i
        return remote(opiece(3, q), opiece(3, q), za.at[i], or_.at[3, q], sp=mate)

    row_arrived(1, 0)
    row_send(1, 0, 2, 4).start()
    row_arrived(2, 1)
    row_send(2, 1, 1, 5).start()
    for j in range(2):
        oload(j).wait()
    for i in range(2):
        own_out(1, i).start()
        own_out(2, i).start()

    zhop(1, 2)
    zhop(2, 1)
    zhop(2, 2)
    send_own(3, inner)
    row_arrived(1, 1)
    twin(1).start()
    row_arrived(2, 0)
    twin(2).start()
    zhop(1, 3)
    send_own(4, inner)

    def project(d, n, p, q):
        left = rows[d : d + n].reshape(n * length, rows.shape[2])
        co = pl.ds(p * wide, (q - p) * wide)
        made = jnp.dot(left, wg[:, co], preferred_element_type=F32).astype(BF)
        y[d : d + n, :, co] = made.reshape(n, length, (q - p) * wide)

    def group(d, p):
        return y[d, :, p * wide : (p + 1) * wide]

    causal = ri >= ci
    tril_short = tril.astype(BF)

    def local(d):
        fl = floor[f]
        logits = group(d, FORGET).astype(F32)
        retain = fl + (1.0 - fl) * jax.nn.sigmoid(logits)
        keys = (1.0 - fl) * jax.nn.sigmoid(-logits)
        step = jnp.log(retain)
        coarse = step.astype(BF)
        fine = (step - coarse.astype(F32)).astype(BF)
        both = jnp.dot(
            tril_short, jnp.concatenate([coarse, fine], axis=1), preferred_element_type=F32
        )
        total = both[:, :wide] + both[:, wide:]
        raw = group(d, QUERY).astype(F32)
        query = raw * jax.nn.sigmoid(raw) * jnp.exp(total)
        value = group(d, VALUE)
        scores = lax.dot_general(
            query.astype(BF), (keys * jnp.exp(-total)).astype(BF), NT, preferred_element_type=F32
        )
        lc = lcol[d]
        gap = lc[:, 0:1] - lrow[d, 0:1, :]
        scores = jnp.where(causal, scores * jnp.exp(jnp.where(causal, gap, 0.0)), 0.0)
        inside[d] = jnp.dot(scores.astype(BF), value, preferred_element_type=F32)
        reach[d] = (query * jnp.exp(lc)).astype(BF)
        full = total + lc
        end = full[length - 1 :, :]
        update = (keys * jnp.exp(end - full)).astype(BF)
        states[d] = lax.dot_general(value, update, TN, preferred_element_type=F32)
        sdecay[d] = jnp.broadcast_to(jnp.exp(end), (8, wide))

    def many(body, first, last):
        def one(d, carry):
            body(d)
            return carry

        lax.fori_loop(first, last, one, 0)

    for load in loads[3:]:
        load.wait()
    twin_arrived(0)
    zready(0)
    zready(1)
    project(0, 1, 0, 2)
    twin_arrived(1)
    twin_arrived(2)
    project(1, 2, 0, 2)
    zhop(1, 4)
    zready(2)
    project(0, 1, 2, 3)
    zhop(2, 3)
    project(1, 2, 2, 3)
    zhop(2, 4)
    row_arrived(3, 0)
    row_arrived(3, 1)
    twin(3).start()
    many(local, 0, 3)
    twin_arrived(3)
    project(3, 1, 0, 2)
    project(3, 1, 2, 3)
    many(local, 3, 4)

    out_arrived(2, order(2, 0))
    relay_out(2, 1).start()
    out_arrived(1, order(1, 0))
    relay_out(1, 2).start()
    own_out(1, 2).start()
    own_out(2, 2).start()

    def state_copy(d):
        return remote(sout.at[d], sin.at[d], ss.at[d], sr.at[d], sp=s + 1)

    def place(j, g):
        return mix.at[:, pl.ds(pl.multiple_of(j * depth + g * wide, wide), wide)]

    def mixed_send(d, j):
        return remote(msend.at[d, j], place(j, f), xs.at[d, j], xr.at[d, j], fs=f ^ d)

    def mixed_arrived(d, j):
        remote(msend.at[d, j], place(j, f ^ d), xs.at[d, j], xr.at[d, j], fs=f ^ 1).wait_recv()

    def deliver(d, j, value):
        if d == 0:
            mix[:, pl.ds(pl.multiple_of(j * depth + f * wide, wide), wide)] = value
        else:
            msend[d, j] = value
            mixed_send(d, j).start()

    def chain(d):
        @pl.when(has_left)
        def _():
            state_copy(d).wait_recv()

        @pl.when(s == 0)
        def _():
            sin[d] = jnp.zeros(sin.shape[1:], BF)

        @pl.when(has_right)
        def _():
            sout[d] = (sin[d].astype(F32) * sdecay[d, 0:1, :] + states[d]).astype(BF)
            state_copy(d).start()

        raw = inside[d] + lax.dot_general(reach[d], sin[d], NT, preferred_element_type=F32)
        scale = lax.rsqrt(jnp.mean(raw * raw, axis=-1, keepdims=True) + 1e-06)
        deliver(d, 1, (raw * scale * hgain[...]).astype(BF))

    turns = (3, 1, 2, 0)
    for d in turns:
        chain(d)


    edge = rim.shape[1]

    def rim_copy(d):
        return remote(
            y.at[d, pl.ds(length - edge, edge), pl.ds(SIGNAL * wide, wide)], rim.at[d],
            ms.at[d], mr.at[d], sp=s + 1,
        )

    zready(3)
    for d in turns:
        project(d, 1, 3, 4)

        @pl.when(has_right)
        def _(d=d):
            rim_copy(d).start()

        @pl.when(s == 0)
        def _(d=d):
            rim[d] = jnp.zeros((edge, wide), BF)

    def filtering(d):
        @pl.when(has_left)
        def _():
            rim_copy(d).wait_recv()

        padded = jnp.concatenate([rim[d], group(d, SIGNAL)], axis=0).astype(F32)
        margin = taps.shape[1] - 1
        filtered = jnp.zeros((length, wide), F32)
        for o in range(margin + 1):
            start = edge - margin + o
            filtered = filtered + taps[f, o : o + 1, :] * padded[start : start + length]
        filt[d] = filtered

    many(filtering, 0, nf)
    zready(4)
    for i in range(2):
        out_arrived(3, 2 * odd + i)
        assist(i).start()
    for d in turns:
        project(d, 1, 4, 5)
        deliver(d, 0, (group(d, GATE).astype(F32) * filt[d]).astype(BF))
    own_out(1, 3).start()
    own_out(2, 3).start()


    def share(i):
        return remote(
            acc.at[i, pl.ds(pl.multiple_of(other * half, half), half), :], orecv.at[i], es.at[i], er.at[i], tp=other
        )

    for d in (1, 2, 3):
        for j in (1, 0):
            mixed_arrived(d, j)

    def begin(i, d, c):
        co = pl.ds(pl.multiple_of(c * 2 * pw, 2 * pw), 2 * pw)
        acc[i] = jnp.dot(mix[...], wo[d, :, co], preferred_element_type=F32)
        share(i).start()

    def finish(i, d, c):
        share(i).wait_recv()
        at = pl.ds(pl.multiple_of((f ^ d) * cols + c * 2 * pw, 2 * pw), 2 * pw)
        out[0, :, at] = (acc[i, pl.ds(pl.multiple_of(t * half, half), half), :] + orecv[i]).astype(BF)

    plan = [
        (0, odd, ()),
        (0, 1 - odd, ()),
        (1, odd, (order(1, 1),)),
        (2, odd, (order(2, 1),)),
        (3, odd, ()),
        (3, 1 - odd, (2 - 2 * odd, 3 - 2 * odd)),
        (1, 1 - odd, (2 - 2 * odd, 3 - 2 * odd)),
        (2, 1 - odd, (2 - 2 * odd, 3 - 2 * odd)),
    ]
    for i, (d, c, waits) in enumerate(plan):
        for q in waits:
            out_arrived(d, q)
        begin(i, d, c)
        if i:
            finish(i - 1, *plan[i - 1][:2])
    finish(len(plan) - 1, *plan[-1][:2])


    for p in range(np_):
        def drained(b, carry, p=p):
            @pl.when(((b < s) & has_right) | ((b > s) & has_left))
            def _():
                relay(b, p, s).wait_send()

            return carry

        lax.fori_loop(0, ns, drained, 0)

        @pl.when(has_right)
        def _(p=p):
            own_right(p).wait_send()

        @pl.when(has_left)
        def _(p=p):
            own_left(p).wait_send()

    for d, j, to_d, slot in ((0, 0, 1, 0), (0, 1, 2, 1), (0, 1, 1, 2), (0, 0, 2, 3), (1, 0, 2, 4), (2, 1, 1, 5)):
        row_send(d, j, to_d, slot).wait_send()
    for to_d in range(1, 3):
        for i in range(4):
            own_out(to_d, i).wait_send()
        relay_out(3 - to_d, to_d).wait_send()
    for i in range(2):
        assist(i).wait_send()
    for d in range(nf):
        twin(d).wait_send()
        if d:
            leak_send(d).wait_send()
            for j in range(2):
                mixed_send(d, j).wait_send()
    for i in range(len(plan)):
        share(i).wait_send()

    @pl.when(has_right)
    def _():
        for d in range(nf):
            state_copy(d).wait_send()
            rim_copy(d).wait_send()


def body(ns, nf, tokens, norm_gain, w0, w1, w2, w3, w4, conv_taps, floor_gate, leak, head_gain, cow, how):
    half, width = tokens.shape[1:]
    length = 2 * half
    heads = leak.shape[2]
    kd = w0.shape[0]
    wide = w0.shape[1] // nf
    assert heads == nf and nf == 4 and floor_gate.shape[0] == heads * wide and ns % 2 == 0
    taps = conv_taps.reshape(conv_taps.shape[0], nf, wide).transpose(1, 0, 2)
    vm = pl.BlockSpec(memory_space=pltpu.VMEM)
    hbm = pl.BlockSpec(memory_space=pltpu.HBM)
    dma = pltpu.SemaphoreType.DMA
    depth, cols = cow.shape
    scratch = [
        pltpu.VMEM((half, width), BF),
        pltpu.VMEM((1, width), F32),
        pltpu.VMEM(taps.shape, F32),
        pltpu.VMEM((heads, 1, wide), F32),
        pltpu.VMEM((heads, length), F32),
        pltpu.VMEM((1, wide), F32),
        pltpu.VMEM((nf, length, width), BF),
        pltpu.VMEM((ns * kd, 5 * wide), BF),
        pltpu.VMEM((nf, length, 5 * wide), BF),
        pltpu.VMEM((nf, 2 * depth, cols), BF),
        pltpu.VMEM((nf, 16, wide), BF),
        pltpu.VMEM((nf, length, wide), F32),
        pltpu.VMEM((nf, length, wide), F32),
        pltpu.VMEM((nf, length, wide), BF),
        pltpu.VMEM((nf, wide, wide), F32),
        pltpu.VMEM((nf, 8, wide), F32),
        pltpu.VMEM((nf, wide, wide), BF),
        pltpu.VMEM((nf, wide, wide), BF),
        pltpu.VMEM((nf, 8, length), F32),
        pltpu.VMEM((nf, length, wide), F32),
        pltpu.VMEM((nf, 8, length), F32),
        pltpu.VMEM((nf, 2, length, wide), BF),
        pltpu.VMEM((length, 2 * depth), BF),
        pltpu.VMEM((2 * nf, length, cols // 2), F32),
        pltpu.VMEM((2 * nf, half, cols // 2), F32),
        dma((6,)), dma((ns, 5)), dma((5,)), dma((ns, 5)), dma((5,)),
        dma((6,)), dma((nf, 2)), dma((nf,)), dma((nf,)), dma((nf,)), dma((nf,)),
        dma((2,)), dma((3, 4)), dma((nf, 4)), dma((3,)), dma((2,)),
        dma((nf, 2)), dma((nf, 2)), dma((nf,)), dma((nf,)), dma((nf,)), dma((nf,)),
        dma((2 * nf,)), dma((2 * nf,)),
    ]
    return pl.pallas_call(
        functools.partial(kernel, ns, nf),
        out_shape=jax.ShapeDtypeStruct(tokens.shape, BF),
        in_specs=[hbm] * 13,
        out_specs=vm,
        scratch_shapes=scratch,
        compiler_params=pltpu.CompilerParams(
            collective_id=0, has_side_effects=True, vmem_limit_bytes=60 * 2**20
        ),
    )(
        tokens, norm_gain[None], w0, w1, w2, w3, w4, taps, floor_gate.reshape(heads, 1, wide),
        leak[0].T, head_gain[None], cow, how,
    )


def solution(mesh):
    in_specs = (
        P("fs", ("sp", "tp"), None),
        P(),
        P("sp", "tp"),
        P("sp", "tp"),
        P("sp", "tp"),
        P("sp", "tp"),
        P("sp", "tp"),
        P(None, "tp"),
        P("tp"),
        P("fs", "sp", "tp"),
        P(),
        P("tp", "fs"),
        P("tp", "fs"),
    )
    out_specs = P("fs", ("sp", "tp"), None)
    step = functools.partial(body, mesh.shape["sp"], mesh.shape["fs"])
    return jax.shard_map(step, mesh=mesh, in_specs=in_specs, out_specs=out_specs, check_vma=False)
```

```python
import functools

import jax
import jax.numpy as jnp
from jax import lax
from jax.experimental import pallas as pl
from jax.experimental.pallas import tpu as pltpu
from jax.sharding import PartitionSpec as P

MESH = pl.DeviceIdType.MESH
BF = jnp.bfloat16
F32 = jnp.float32
NT = (((1,), (1,)), ((), ()))
TN = (((0,), (0,)), ((), ()))
GATE, SIGNAL, QUERY, FORGET, VALUE = 4, 3, 1, 0, 2


def kernel(
    ns, nf,
    tok_h, gain_h, w0, w1, w2, w3, w4, taps_h, floor_h, leak_h, hgain_h, cow, how,
    out,
    tokv, gain, taps, floor, leak_t, hgain,
    rows, wg, y, wo, brim, rim, filt, inside, reach, states, sdecay, sin, sout,
    lk, lcol, lrow, msend, mix, acc, orecv, done,
    il, zs, zsl, zr, zloc, rs, rr, ts, tr, ls, lr, oloc, os_, or_, ov, zc, xs, xr, ms, mr, ss, sr, es, er, fin,
):
    s, f, t = lax.axis_index("sp"), lax.axis_index("fs"), lax.axis_index("tp")
    other = 1 - t
    half = tokv.shape[0]
    length = 2 * half
    kd = w0.shape[0]
    wide = w0.shape[1] // nf
    ws = (w3, w2, w4, w1, w0)
    np_ = len(ws)
    has_left, has_right = s > 0, s < ns - 1
    inner = has_left & has_right
    outs = (cow, how)
    depth, cols = cow.shape
    odd = lax.rem(s, 2)
    mate = s + 1 - 2 * odd

    def remote(src, dst, send, recv, **where):
        return pltpu.make_async_remote_copy(
            src_ref=src, dst_ref=dst, send_sem=send, recv_sem=recv,
            device_id=where, device_id_type=MESH,
        )


    def wblock(b, p):
        return wg.at[pl.ds(pl.multiple_of(b * kd, kd), kd), pl.ds(p * wide, wide)]

    def wload(p):
        return pltpu.make_async_copy(
            ws[p].at[:, pl.ds(pl.multiple_of(f * wide, wide), wide)], wblock(s, p), zloc.at[p]
        )

    def oload(j):
        return pltpu.make_async_copy(outs[j], wo.at[0, pl.ds(j * depth, depth), :], oloc.at[0])

    loads = [
        pltpu.make_async_copy(src, dst, il.at[i])
        for i, (src, dst) in enumerate(
            ((tok_h.at[0], tokv), (gain_h, gain), (leak_h, leak_t), (taps_h, taps), (floor_h, floor), (hgain_h, hgain))
        )
    ]

    wload(0).start()
    loads[0].start()
    wload(1).start()
    for load in loads[1:]:
        load.start()
    for p in range(2, np_):
        wload(p).start()
    for j in range(2):
        oload(j).start()

    barrier = pltpu.get_barrier_semaphore()
    for d in range(nf - 1, 0, -1):
        pl.semaphore_signal(barrier, inc=1, device_id={"fs": f ^ d}, device_id_type=MESH)

    @pl.when(has_left)
    def _():
        pl.semaphore_signal(barrier, inc=1, device_id={"sp": s - 1}, device_id_type=MESH)

    @pl.when(has_right)
    def _():
        pl.semaphore_signal(barrier, inc=1, device_id={"sp": s + 1}, device_id_type=MESH)

    pl.semaphore_signal(barrier, inc=1, device_id={"tp": other}, device_id_type=MESH)


    for load in loads[:3]:
        load.wait()
    lk[0, pl.ds(0, leak_t.shape[0]), :] = leak_t[...]
    x = tokv[...].astype(F32)
    center = x - jnp.mean(x, axis=-1, keepdims=True)
    spread = jnp.mean(center * center, axis=-1, keepdims=True)
    rows[0, pl.ds(pl.multiple_of(t * half, half), half), :] = (
        center * lax.rsqrt(spread + 1e-05) * gain[...]
    ).astype(BF)

    ends = jnp.where(has_left, 1, 0) + jnp.where(has_right, 1, 0)
    pl.semaphore_wait(barrier, nf + ends)


    def own_right(p):
        return remote(wblock(s, p), wblock(s, p), zs.at[0], zr.at[s, p], sp=s + 1)

    def own_left(p):
        return remote(wblock(s, p), wblock(s, p), zsl.at[0], zr.at[s, p], sp=s - 1)

    def relay(b, p, to):
        return remote(wblock(b, p), wblock(b, p), zs.at[0], zr.at[b, p], sp=to)

    def send_own(p, where):
        @pl.when(where & has_right)
        def _():
            own_right(p).start()

        @pl.when(where & has_left)
        def _():
            own_left(p).start()

    def zhop(k, p):
        @pl.when((s - k >= 0) & has_right)
        def _():
            relay(s - k, p, s + 1).wait_recv()
            relay(s - k, p, s + 1).start()

        @pl.when((s + k < ns) & has_left)
        def _():
            relay(s + k, p, s - 1).wait_recv()
            relay(s + k, p, s - 1).start()

    def zready(p):
        def far(k, carry):
            zhop(k, p)
            return carry

        if ns > 3:
            lax.fori_loop(3, ns, far, 0)

        def hop(k, carry):
            @pl.when((s - k >= 0) & (s == ns - 1))
            def _():
                relay(s - k, p, s - 1).wait_recv()

            @pl.when((s + k < ns) & (s == 0))
            def _():
                relay(s + k, p, s + 1).wait_recv()

            return carry

        lax.fori_loop(1, ns, hop, 0)

    always = s >= 0
    for p in range(2):
        wload(p).wait()
        send_own(p, always)

    quarter = half // 2

    def piece(d, j):
        return rows.at[d, pl.ds(pl.multiple_of(t * half + j * quarter, quarter), quarter), :]

    def core_rows(d, core):
        return rows.at[d, pl.ds(pl.multiple_of(core * half, half), half), :]

    def row_send(d, j, to_d):
        return remote(piece(d, j), piece(d ^ to_d, j), rs.at[0], rr.at[(d ^ to_d) - 1, j], fs=f ^ to_d)

    def row_arrived(d, j):
        remote(piece(d, j), piece(d, j), rs.at[0], rr.at[d - 1, j], fs=f ^ 1).wait_recv()

    def twin(d):
        return remote(core_rows(d, t), core_rows(d, t), ts.at[0], tr.at[d], tp=other)

    def twin_arrived(d):
        remote(core_rows(d, other), core_rows(d, other), ts.at[0], tr.at[d], tp=other).wait_recv()

    def leak_send(d):
        return remote(lk.at[0], lk.at[d], ls.at[0], lr.at[0], fs=f ^ d)

    for d in range(1, nf):
        leak_send(d).start()
    row_send(0, 0, 1).start()
    row_send(0, 1, 2).start()
    row_send(0, 1, 1).start()
    row_send(0, 0, 2).start()
    twin(0).start()
    for p in range(2, np_):
        wload(p).wait()
        send_own(p, jnp.logical_not(inner))

    zhop(1, 0)
    zhop(1, 1)


    others = lk.at[pl.ds(1, nf - 1)]
    remote(others, others, ls.at[0], lr.at[0], fs=f ^ 1).wait_recv()
    ri = lax.broadcasted_iota(jnp.int32, (length, length), 0)
    ci = lax.broadcasted_iota(jnp.int32, (length, length), 1)
    tril = (ri >= ci).astype(F32)
    triu = (ri <= ci).astype(F32)
    high = lax.Precision.HIGHEST
    head_leak = jnp.concatenate(
        [lk[d, pl.ds(f, 1), :] for d in range(nf)] + [jnp.zeros((8 - nf, length), F32)], axis=0
    )
    lsum = lax.dot_general(tril, head_leak, NT, precision=high, preferred_element_type=F32)
    lsum_t = jnp.dot(head_leak, triu, precision=high, preferred_element_type=F32)
    for d in range(nf):
        lcol[d] = jnp.broadcast_to(lsum[:, d : d + 1], (length, wide))
        lrow[d] = jnp.broadcast_to(lsum_t[d : d + 1, :], (8, length))

    zhop(2, 0)
    send_own(2, inner)


    pw = cols // 4

    full = (0, 2 * depth)

    def opiece(d, q, part=full):
        return wo.at[d, pl.ds(*part), pl.ds(pl.multiple_of(q * pw, pw), pw)]

    def order(to_d, i):
        low, high = 2 * odd, 2 - 2 * odd
        return ((low + 1, low, high, high + 1) if to_d == 1 else (low, low + 1, high + 1, high))[i]

    lower, upper = (0, depth), (depth, depth)

    def own_out(to_d, i, part=full):
        q = order(to_d, i)
        return remote(opiece(0, q, part), opiece(to_d, q, part), os_.at[0], or_.at[to_d - 1, q], fs=f ^ to_d)

    def out_arrived(d, q, part=full):
        remote(opiece(d, q, part), opiece(d, q, part), os_.at[0], or_.at[d - 1, q], fs=f ^ 1).wait_recv()

    def third_upper(to_d):
        q = order(to_d, 2)
        return remote(opiece(0, q, upper), opiece(to_d, q, upper), os_.at[0], ov.at[to_d - 1], fs=f ^ to_d)

    def third_lower(to_d):
        return own_out(to_d, 2, lower)

    taken = (depth, depth // 2)

    def fourth(to_d, side):
        return own_out(to_d, 3, (taken[side], 2 * depth - taken[side]))

    def swap(d, side):
        q, part = order(d, 0), (0, taken[1 - side])
        return remote(opiece(d, q, part), opiece(d, q, part), os_.at[0], zc.at[d - 1], sp=mate)

    def swapped(d, side):
        q, part = order(d, 3), (0, taken[side])
        remote(opiece(d, q, part), opiece(d, q, part), os_.at[0], zc.at[d - 1], sp=mate).wait_recv()

    def by_side(work):
        for side in range(2):
            @pl.when(odd == side)
            def _(side=side):
                work(side)

    def relay_out(d, to_d):
        q = order(d, 0)
        return remote(opiece(d, q), opiece(3, q), os_.at[0], or_.at[2, q], fs=f ^ to_d)

    def assist(i):
        q = 2 * odd + i
        return remote(opiece(3, q), opiece(3, q), os_.at[0], or_.at[2, q], sp=mate)

    row_arrived(1, 0)
    row_send(1, 0, 2).start()
    row_arrived(2, 1)
    row_send(2, 1, 1).start()
    pltpu.make_async_copy(wo.at[0], wo.at[0], oloc.at[0]).wait()
    for i in range(2):
        own_out(1, i).start()
        own_out(2, i).start()

    zhop(1, 2)
    zhop(2, 1)
    zhop(2, 2)
    send_own(3, inner)
    row_arrived(1, 1)
    twin(1).start()
    row_arrived(2, 0)
    twin(2).start()
    zhop(1, 3)
    send_own(4, inner)

    def project(d, n, p, q):
        left = rows[pl.ds(d, n)].reshape(n * length, rows.shape[2])
        co = pl.ds(p * wide, (q - p) * wide)
        made = jnp.dot(left, wg[:, co], preferred_element_type=F32).astype(BF)
        y[pl.ds(d, n), :, co] = made.reshape(n, length, (q - p) * wide)

    def group(d, p):
        return y[d, :, p * wide : (p + 1) * wide]

    causal = ri >= ci
    tril_short = tril.astype(BF)

    def local(d):
        fl = floor[f]
        logits = group(d, FORGET).astype(F32)
        retain = fl + (1.0 - fl) * jax.nn.sigmoid(logits)
        keys = (1.0 - fl) * jax.nn.sigmoid(-logits)
        step = jnp.log(retain)
        coarse = step.astype(BF)
        fine = (step - coarse.astype(F32)).astype(BF)
        both = jnp.dot(
            tril_short, jnp.concatenate([coarse, fine], axis=1), preferred_element_type=F32
        )
        total = both[:, :wide] + both[:, wide:]
        raw = group(d, QUERY).astype(F32)
        query = raw * jax.nn.sigmoid(raw) * jnp.exp(total)
        value = group(d, VALUE)
        scores = lax.dot_general(
            query.astype(BF), (keys * jnp.exp(-total)).astype(BF), NT, preferred_element_type=F32
        )
        lc = lcol[d]
        gap = lc[:, 0:1] - lrow[d, 0:1, :]
        scores = jnp.where(causal, scores * jnp.exp(jnp.where(causal, gap, 0.0)), 0.0)
        inside[d] = jnp.dot(scores.astype(BF), value, preferred_element_type=F32)
        reach[d] = (query * jnp.exp(lc)).astype(BF)
        full = total + lc
        end = full[length - 1 :, :]
        update = (keys * jnp.exp(end - full)).astype(BF)
        states[d] = lax.dot_general(value, update, TN, preferred_element_type=F32)
        sdecay[d] = jnp.broadcast_to(jnp.exp(end), (8, wide))

    def many(body, first, last):
        def one(d, carry):
            body(d)
            return carry

        lax.fori_loop(first, last, one, 0)

    for load in loads[3:]:
        load.wait()
    twin_arrived(0)
    zready(0)
    zready(1)
    project(0, 1, 0, 2)
    twin_arrived(1)
    twin_arrived(2)
    project(1, 2, 0, 2)
    zready(2)
    project(0, 1, 2, 3)
    project(1, 2, 2, 3)
    row_arrived(3, 0)
    row_arrived(3, 1)
    twin(3).start()
    many(local, 0, 3)
    zhop(1, 4)
    zhop(2, 3)
    zhop(2, 4)
    twin_arrived(3)
    project(3, 1, 0, 2)
    project(3, 1, 2, 3)
    many(local, 3, 4)

    out_arrived(2, order(2, 0))
    relay_out(2, 1).start()
    out_arrived(1, order(1, 0))
    relay_out(1, 2).start()

    def state_copy(d):
        return remote(sout.at[d], sin.at[d], ss.at[0], sr.at[d], sp=s + 1)

    def place(j, g):
        return mix.at[:, pl.ds(pl.multiple_of(j * depth + g * wide, wide), wide)]

    def mixed_send(d, j):
        return remote(msend.at[d - 1, j], place(j, f), xs.at[0], xr.at[0], fs=f ^ d)

    def deliver(d, j, value):
        if d == 0:
            mix[:, pl.ds(pl.multiple_of(j * depth + f * wide, wide), wide)] = value
        else:
            msend[d - 1, j] = value
            mixed_send(d, j).start()

    def chain(d):
        @pl.when(has_left)
        def _():
            state_copy(d).wait_recv()

        @pl.when(s == 0)
        def _():
            sin[d] = jnp.zeros(sin.shape[1:], BF)

        @pl.when(has_right)
        def _():
            sout[d] = (sin[d].astype(F32) * sdecay[d, 0:1, :] + states[d]).astype(BF)
            state_copy(d).start()

        raw = inside[d] + lax.dot_general(reach[d], sin[d], NT, preferred_element_type=F32)
        scale = lax.rsqrt(jnp.mean(raw * raw, axis=-1, keepdims=True) + 1e-06)
        deliver(d, 1, (raw * scale * hgain[...]).astype(BF))

    turns = (3, 1, 2, 0)
    last = s == ns - 1
    inland = jnp.logical_not(last)


    edge = rim.shape[1]

    def rim_copy():
        return remote(brim, rim, ms.at[0], mr.at[0], sp=s + 1)

    def swaps(side):
        for d in (1, 2):
            swap(d, side).start()

    def signal():
        zready(3)

        @pl.when(has_right)
        def _():
            ends_ = rows[:, pl.ds(length - edge, edge), :].reshape(nf * edge, rows.shape[2])
            made = jnp.dot(ends_, wg[:, pl.ds(SIGNAL * wide, wide)], preferred_element_type=F32).astype(BF)
            brim[...] = made.reshape(nf, edge, wide)
            rim_copy().start()

        @pl.when(s == 0)
        def _():
            rim[...] = jnp.zeros(rim.shape, BF)

        @pl.when((odd == 0) & (s > 0))
        def _():
            swaps(0)

        def one(d, carry):
            project(d, 1, 3, 4)
            return carry

        lax.fori_loop(0, nf, one, 0)

    def assists():
        for i in range(2):
            out_arrived(3, 2 * odd + i)
            assist(i).start()

    @pl.when(odd == 1)
    def _():
        swaps(1)

    def thirds():
        for to_d in (1, 2):
            third_upper(to_d).start()

    @pl.when(last)
    def _():
        thirds()
        signal()
        assists()

    for d in turns:
        chain(d)

    @pl.when(s == 0)
    def _():
        swaps(0)

    @pl.when(inland)
    def _():
        thirds()
        signal()

    @pl.when(inland)
    def _():
        assists()


    @pl.when(has_left)
    def _():
        rim_copy().wait_recv()

    def filtering(d):
        padded = jnp.concatenate([rim[d], group(d, SIGNAL)], axis=0).astype(F32)
        margin = taps.shape[1] - 1
        filtered = jnp.zeros((length, wide), F32)
        for o in range(margin + 1):
            start = edge - margin + o
            filtered = filtered + taps[f, o : o + 1, :] * padded[start : start + length]
        filt[d] = filtered

    many(filtering, 0, nf)
    zready(4)
    for d in turns:
        project(d, 1, 4, 5)
        deliver(d, 0, (group(d, GATE).astype(F32) * filt[d]).astype(BF))
    for to_d in (1, 2):
        third_lower(to_d).start()

    def fourths(side):
        for to_d in (1, 2):
            fourth(to_d, side).start()

    by_side(fourths)


    def share(i):
        return remote(
            acc.at[i, pl.ds(pl.multiple_of(other * half, half), half), :], orecv.at[i], es.at[0], er.at[i], tp=other
        )

    mixed = remote(msend, msend, xs.at[0], xr.at[0], fs=f ^ 1)
    mixed.wait_recv()

    def begin(i, d, c):
        co = pl.ds(pl.multiple_of(c * 2 * pw, 2 * pw), 2 * pw)
        acc[i] = jnp.dot(mix[...], wo[d, :, co], preferred_element_type=F32)
        share(i).start()

    def finish(i, d, c):
        share(i).wait_recv()
        at = pl.ds(pl.multiple_of((f ^ d) * cols + c * 2 * pw, 2 * pw), 2 * pw)
        done[:, at] = (acc[i, pl.ds(pl.multiple_of(t * half, half), half), :] + orecv[i]).astype(BF)
        store(i, d, c).start()

    def store(i, d, c):
        at = pl.ds(pl.multiple_of((f ^ d) * cols + c * 2 * pw, 2 * pw), 2 * pw)
        return pltpu.make_async_copy(done.at[:, at], out.at[0, :, at], fin.at[0])

    def last_quarters(d):
        third_upper(d).wait_recv()
        out_arrived(d, order(d, 2), lower)

        def rest(side):
            swapped(d, side)
            out_arrived(d, order(d, 3), (taken[side], 2 * depth - taken[side]))

        by_side(rest)

    def assisted(d):
        for q in (2 - 2 * odd, 3 - 2 * odd):
            out_arrived(3, q)

    lag = 3
    plan = [
        (0, odd, None),
        (0, 1 - odd, None),
        (1, odd, lambda d: out_arrived(d, order(d, 1))),
        (2, odd, lambda d: out_arrived(d, order(d, 1))),
        (3, odd, None),
        (1, 1 - odd, last_quarters),
        (2, 1 - odd, last_quarters),
        (3, 1 - odd, assisted),
    ]
    for i, (d, c, ready) in enumerate(plan):
        if ready:
            ready(d)
        begin(i, d, c)
        if i >= lag:
            finish(i - lag, *plan[i - lag][:2])
    for i in range(len(plan) - lag, len(plan)):
        finish(i, *plan[i][:2])


    def drained(ref, sem):
        pltpu.make_async_copy(ref, ref, sem).wait()

    @pl.when(inner)
    def _():
        drained(wg, zs.at[0])

    own_rows = wg.at[pl.ds(pl.multiple_of(s * kd, kd), kd), :]

    @pl.when(s == 0)
    def _():
        drained(own_rows, zs.at[0])

    @pl.when(has_left)
    def _():
        drained(own_rows, zsl.at[0])

    drained(rows.at[pl.ds(0, 3), pl.ds(0, half), :], rs.at[0])
    drained(rows.at[:, pl.ds(0, half), :], ts.at[0])
    drained(others, ls.at[0])
    drained(msend, xs.at[0])
    drained(orecv, es.at[0])
    drained(done, fin.at[0])

    def quarters(side):
        count = 2 * (8 * depth - taken[side]) + 8 * depth + 2 * taken[1 - side]
        drained(wo.at[:, pl.ds(0, count // 16), :], os_.at[0])

    by_side(quarters)

    @pl.when(has_right)
    def _():
        drained(sout, ss.at[0])
        drained(brim, ms.at[0])


def body(ns, nf, tokens, norm_gain, w0, w1, w2, w3, w4, conv_taps, floor_gate, leak, head_gain, cow, how):
    half, width = tokens.shape[1:]
    length = 2 * half
    heads = leak.shape[2]
    kd = w0.shape[0]
    wide = w0.shape[1] // nf
    assert heads == nf and nf == 4 and floor_gate.shape[0] == heads * wide and ns % 2 == 0
    taps = conv_taps.reshape(conv_taps.shape[0], nf, wide).transpose(1, 0, 2)
    hbm = pl.BlockSpec(memory_space=pltpu.HBM)
    dma = pltpu.SemaphoreType.DMA
    depth, cols = cow.shape
    scratch = [
        pltpu.VMEM((half, width), BF),
        pltpu.VMEM((1, width), F32),
        pltpu.VMEM(taps.shape, F32),
        pltpu.VMEM((heads, 1, wide), F32),
        pltpu.VMEM((heads, length), F32),
        pltpu.VMEM((1, wide), F32),
        pltpu.VMEM((nf, length, width), BF),
        pltpu.VMEM((ns * kd, 5 * wide), BF),
        pltpu.VMEM((nf, length, 5 * wide), BF),
        pltpu.VMEM((nf, 2 * depth, cols), BF),
        pltpu.VMEM((nf, 16, wide), BF),
        pltpu.VMEM((nf, 16, wide), BF),
        pltpu.VMEM((nf, length, wide), F32),
        pltpu.VMEM((nf, length, wide), F32),
        pltpu.VMEM((nf, length, wide), BF),
        pltpu.VMEM((nf, wide, wide), F32),
        pltpu.VMEM((nf, 8, wide), F32),
        pltpu.VMEM((nf, wide, wide), BF),
        pltpu.VMEM((nf, wide, wide), BF),
        pltpu.VMEM((nf, 8, length), F32),
        pltpu.VMEM((nf, length, wide), F32),
        pltpu.VMEM((nf, 8, length), F32),
        pltpu.VMEM((nf - 1, 2, length, wide), BF),
        pltpu.VMEM((length, 2 * depth), BF),
        pltpu.VMEM((2 * nf, length, cols // 2), F32),
        pltpu.VMEM((2 * nf, half, cols // 2), F32),
        pltpu.VMEM((half, width), BF),
        dma((6,)), dma((1,)), dma((1,)), dma((ns, 5)), dma((5,)),
        dma((1,)), dma((nf - 1, 2)), dma((1,)), dma((nf,)), dma((1,)), dma((1,)),
        dma((1,)), dma((1,)), dma((3, 4)), dma((2,)), dma((2,)),
        dma((1,)), dma((1,)), dma((1,)), dma((1,)), dma((1,)), dma((nf,)),
        dma((1,)), dma((2 * nf,)), dma((1,)),
    ]
    return pl.pallas_call(
        functools.partial(kernel, ns, nf),
        out_shape=jax.ShapeDtypeStruct(tokens.shape, BF),
        in_specs=[hbm] * 13,
        out_specs=hbm,
        scratch_shapes=scratch,
        compiler_params=pltpu.CompilerParams(
            collective_id=0, has_side_effects=True, vmem_limit_bytes=60 * 2**20
        ),
    )(
        tokens, norm_gain[None], w0, w1, w2, w3, w4, taps, floor_gate.reshape(heads, 1, wide),
        leak[0].T, head_gain[None], cow, how,
    )


def solution(mesh):
    in_specs = (
        P("fs", ("sp", "tp"), None),
        P(),
        P("sp", "tp"),
        P("sp", "tp"),
        P("sp", "tp"),
        P("sp", "tp"),
        P("sp", "tp"),
        P(None, "tp"),
        P("tp"),
        P("fs", "sp", "tp"),
        P(),
        P("tp", "fs"),
        P("tp", "fs"),
    )
    out_specs = P("fs", ("sp", "tp"), None)
    step = functools.partial(body, mesh.shape["sp"], mesh.shape["fs"])
    return jax.shard_map(step, mesh=mesh, in_specs=in_specs, out_specs=out_specs, check_vma=False)
```

```python
import functools

import jax
import jax.numpy as jnp
from jax import lax
from jax.experimental import pallas as pl
from jax.experimental.pallas import tpu as pltpu
from jax.sharding import PartitionSpec as P

MESH = pl.DeviceIdType.MESH
BF = jnp.bfloat16
F32 = jnp.float32
NT = (((1,), (1,)), ((), ()))
TN = (((0,), (0,)), ((), ()))
GATE, SIGNAL, QUERY, FORGET, VALUE = 4, 3, 1, 0, 2


def kernel(
    ns, nf,
    tok_h, gain_h, w0, w1, w2, w3, w4, taps_h, floor_h, leak_h, hgain_h, cow, how,
    part, twin_part,
    tokv, gain, taps, floor, leak_t, hgain,
    rows, wg, y, wo, brim, rim, filt, inside, reach, states, sdecay, sin, sout,
    lk, lcol, lrow, msend, mix, shares,
    il, zs, zsl, zr, zloc, rs, rr, ts, tr, ls, lr, oloc, os_, or_, ov, zc, xs, xr, ms, mr, ss, sr, es, er, fin,
):
    s, f, t = lax.axis_index("sp"), lax.axis_index("fs"), lax.axis_index("tp")
    other = 1 - t
    half = tokv.shape[0]
    length = 2 * half
    kd = w0.shape[0]
    wide = w0.shape[1] // nf
    ws = (w3, w2, w4, w1, w0)
    np_ = len(ws)
    has_left, has_right = s > 0, s < ns - 1
    inner = has_left & has_right
    outs = (cow, how)
    depth, cols = cow.shape
    odd = lax.rem(s, 2)
    mate = s + 1 - 2 * odd

    def remote(src, dst, send, recv, **where):
        return pltpu.make_async_remote_copy(
            src_ref=src, dst_ref=dst, send_sem=send, recv_sem=recv,
            device_id=where, device_id_type=MESH,
        )


    def wblock(b, p):
        return wg.at[pl.ds(pl.multiple_of(b * kd, kd), kd), pl.ds(p * wide, wide)]

    def wload(p):
        return pltpu.make_async_copy(
            ws[p].at[:, pl.ds(pl.multiple_of(f * wide, wide), wide)], wblock(s, p), zloc.at[p]
        )

    def oload(j):
        return pltpu.make_async_copy(outs[j], wo.at[0, pl.ds(j * depth, depth), :], oloc.at[0])

    quarter = half // 2
    pieces = [pl.ds(j * quarter, quarter) for j in range(2)]
    loads = [
        pltpu.make_async_copy(src, dst, il.at[i])
        for i, (src, dst) in enumerate(
            (
                (tok_h.at[0, pieces[0]], tokv.at[pieces[0]]), (gain_h, gain), (tok_h.at[0, pieces[1]], tokv.at[pieces[1]]),
                (leak_h, leak_t), (taps_h, taps), (floor_h, floor), (hgain_h, hgain),
            )
        )
    ]

    barrier = pltpu.get_barrier_semaphore()
    for d in range(nf - 1, 0, -1):
        pl.semaphore_signal(barrier, inc=1, device_id={"fs": f ^ d}, device_id_type=MESH)

    @pl.when(has_left)
    def _():
        pl.semaphore_signal(barrier, inc=1, device_id={"sp": s - 1}, device_id_type=MESH)

    @pl.when(has_right)
    def _():
        pl.semaphore_signal(barrier, inc=1, device_id={"sp": s + 1}, device_id_type=MESH)

    pl.semaphore_signal(barrier, inc=1, device_id={"tp": other}, device_id_type=MESH)

    for load in loads[:4]:
        load.start()
    wload(0).start()
    wload(1).start()
    for load in loads[4:]:
        load.start()
    for p in range(2, np_):
        wload(p).start()
    for j in range(2):
        oload(j).start()


    loads[3].wait()
    lk[0, pl.ds(0, leak_t.shape[0]), :] = leak_t[...]

    def normalize(j):
        for load in loads[2 * j : 2 + j]:
            load.wait()
        x = tokv[pieces[j]].astype(F32)
        center = x - jnp.mean(x, axis=-1, keepdims=True)
        spread = jnp.mean(center * center, axis=-1, keepdims=True)
        rows[0, pl.ds(pl.multiple_of(t * half + j * quarter, quarter), quarter), :] = (
            center * lax.rsqrt(spread + 1e-05) * gain[...]
        ).astype(BF)

    normalize(0)
    ends = jnp.where(has_left, 1, 0) + jnp.where(has_right, 1, 0)
    pl.semaphore_wait(barrier, nf + ends)


    def own_right(p):
        return remote(wblock(s, p), wblock(s, p), zs.at[0], zr.at[s, p], sp=s + 1)

    def own_left(p):
        return remote(wblock(s, p), wblock(s, p), zsl.at[0], zr.at[s, p], sp=s - 1)

    def relay(b, p, to):
        return remote(wblock(b, p), wblock(b, p), zs.at[0], zr.at[b, p], sp=to)

    def send_own(p, where):
        @pl.when(where & has_right)
        def _():
            own_right(p).start()

        @pl.when(where & has_left)
        def _():
            own_left(p).start()

    def zhop(k, p):
        @pl.when((s - k >= 0) & has_right)
        def _():
            relay(s - k, p, s + 1).wait_recv()
            relay(s - k, p, s + 1).start()

        @pl.when((s + k < ns) & has_left)
        def _():
            relay(s + k, p, s - 1).wait_recv()
            relay(s + k, p, s - 1).start()

    def zready(p):
        def far(k, carry):
            zhop(k, p)
            return carry

        if ns > 3:
            lax.fori_loop(3, ns, far, 0)

        def hop(k, carry):
            @pl.when((s - k >= 0) & (s == ns - 1))
            def _():
                relay(s - k, p, s - 1).wait_recv()

            @pl.when((s + k < ns) & (s == 0))
            def _():
                relay(s + k, p, s + 1).wait_recv()

            return carry

        lax.fori_loop(1, ns, hop, 0)

    always = s >= 0
    for p in range(2):
        wload(p).wait()
        send_own(p, always)

    def piece(d, j):
        return rows.at[d, pl.ds(pl.multiple_of(t * half + j * quarter, quarter), quarter), :]

    def core_rows(d, core):
        return rows.at[d, pl.ds(pl.multiple_of(core * half, half), half), :]

    def row_send(d, j, to_d):
        return remote(piece(d, j), piece(d ^ to_d, j), rs.at[0], rr.at[(d ^ to_d) - 1, j], fs=f ^ to_d)

    def row_arrived(d, j):
        remote(piece(d, j), piece(d, j), rs.at[0], rr.at[d - 1, j], fs=f ^ 1).wait_recv()

    def twin(d):
        return remote(core_rows(d, t), core_rows(d, t), ts.at[0], tr.at[d], tp=other)

    def twin_arrived(d):
        remote(core_rows(d, other), core_rows(d, other), ts.at[0], tr.at[d], tp=other).wait_recv()

    def leak_send(d):
        return remote(lk.at[0], lk.at[d], ls.at[0], lr.at[0], fs=f ^ d)

    for d in range(1, nf):
        leak_send(d).start()
    row_send(0, 0, 1).start()
    normalize(1)
    row_send(0, 1, 2).start()
    row_send(0, 1, 1).start()
    row_send(0, 0, 2).start()
    twin(0).start()
    for p in range(2, np_):
        wload(p).wait()
        send_own(p, jnp.logical_not(inner))

    zhop(1, 0)
    zhop(1, 1)


    others = lk.at[pl.ds(1, nf - 1)]
    remote(others, others, ls.at[0], lr.at[0], fs=f ^ 1).wait_recv()
    ri = lax.broadcasted_iota(jnp.int32, (length, length), 0)
    ci = lax.broadcasted_iota(jnp.int32, (length, length), 1)
    tril = (ri >= ci).astype(F32)
    triu = (ri <= ci).astype(F32)
    high = lax.Precision.HIGHEST
    head_leak = jnp.concatenate(
        [lk[d, pl.ds(f, 1), :] for d in range(nf)] + [jnp.zeros((8 - nf, length), F32)], axis=0
    )
    lsum = lax.dot_general(tril, head_leak, NT, precision=high, preferred_element_type=F32)
    lsum_t = jnp.dot(head_leak, triu, precision=high, preferred_element_type=F32)
    for d in range(nf):
        lcol[d] = jnp.broadcast_to(lsum[:, d : d + 1], (length, wide))
        lrow[d] = jnp.broadcast_to(lsum_t[d : d + 1, :], (8, length))

    zhop(2, 0)
    send_own(2, inner)


    pw = cols // 4

    full = (0, 2 * depth)

    def opiece(d, q, part=full):
        return wo.at[d, pl.ds(*part), pl.ds(pl.multiple_of(q * pw, pw), pw)]

    def order(to_d, i):
        low, high = 2 * odd, 2 - 2 * odd
        return ((low + 1, low, high, high + 1) if to_d == 1 else (low, low + 1, high + 1, high))[i]

    lower, upper = (0, depth), (depth, depth)

    def own_out(to_d, i, part=full):
        q = order(to_d, i)
        return remote(opiece(0, q, part), opiece(to_d, q, part), os_.at[0], or_.at[to_d - 1, q], fs=f ^ to_d)

    def out_arrived(d, q, part=full):
        remote(opiece(d, q, part), opiece(d, q, part), os_.at[0], or_.at[d - 1, q], fs=f ^ 1).wait_recv()

    def third_upper(to_d):
        q = order(to_d, 2)
        return remote(opiece(0, q, upper), opiece(to_d, q, upper), os_.at[0], ov.at[to_d - 1], fs=f ^ to_d)

    def third_lower(to_d):
        return own_out(to_d, 2, lower)

    def taken(side, core):
        return depth * (3 - 2 * core) // (2 + 2 * side)

    def fourth(to_d, side, core):
        return own_out(to_d, 3, (taken(side, core), 2 * depth - taken(side, core)))

    def swap(d, side, core):
        q, part = order(d, 0), (0, taken(1 - side, core))
        return remote(opiece(d, q, part), opiece(d, q, part), os_.at[0], zc.at[d - 1], sp=mate)

    def swapped(d, side, core):
        q, part = order(d, 3), (0, taken(side, core))
        remote(opiece(d, q, part), opiece(d, q, part), os_.at[0], zc.at[d - 1], sp=mate).wait_recv()

    def by_side(work):
        for side in range(2):
            for core in range(2):
                @pl.when((odd == side) & (t == core))
                def _(side=side, core=core):
                    work(side, core)

    def relay_out(d, to_d):
        q = order(d, 0)
        return remote(opiece(d, q), opiece(3, q), os_.at[0], or_.at[2, q], fs=f ^ to_d)

    def assist(i):
        q = 2 * odd + i
        return remote(opiece(3, q), opiece(3, q), os_.at[0], or_.at[2, q], sp=mate)

    row_arrived(1, 0)
    row_send(1, 0, 2).start()
    row_arrived(2, 1)
    row_send(2, 1, 1).start()
    pltpu.make_async_copy(wo.at[0], wo.at[0], oloc.at[0]).wait()
    for i in range(2):
        own_out(1, i).start()
        own_out(2, i).start()

    zhop(1, 2)
    zhop(2, 1)
    zhop(2, 2)
    send_own(3, inner)
    row_arrived(1, 1)
    twin(1).start()
    row_arrived(2, 0)
    twin(2).start()
    zhop(1, 3)
    send_own(4, inner)

    def project(d, n, p, q):
        left = rows[pl.ds(d, n)].reshape(n * length, rows.shape[2])
        co = pl.ds(p * wide, (q - p) * wide)
        made = jnp.dot(left, wg[:, co], preferred_element_type=F32).astype(BF)
        y[pl.ds(d, n), :, co] = made.reshape(n, length, (q - p) * wide)

    def group(d, p):
        return y[d, :, p * wide : (p + 1) * wide]

    causal = ri >= ci
    tril_short = tril.astype(BF)

    def local(d):
        fl = floor[f]
        logits = group(d, FORGET).astype(F32)
        retain = fl + (1.0 - fl) * jax.nn.sigmoid(logits)
        keys = (1.0 - fl) * jax.nn.sigmoid(-logits)
        step = jnp.log(retain)
        coarse = step.astype(BF)
        fine = (step - coarse.astype(F32)).astype(BF)
        both = jnp.dot(
            tril_short, jnp.concatenate([coarse, fine], axis=1), preferred_element_type=F32
        )
        total = both[:, :wide] + both[:, wide:]
        raw = group(d, QUERY).astype(F32)
        query = raw * jax.nn.sigmoid(raw) * jnp.exp(total)
        value = group(d, VALUE)
        scores = lax.dot_general(
            query.astype(BF), (keys * jnp.exp(-total)).astype(BF), NT, preferred_element_type=F32
        )
        lc = lcol[d]
        gap = lc[:, 0:1] - lrow[d, 0:1, :]
        scores = jnp.where(causal, scores * jnp.exp(jnp.where(causal, gap, 0.0)), 0.0)
        inside[d] = jnp.dot(scores.astype(BF), value, preferred_element_type=F32)
        reach[d] = (query * jnp.exp(lc)).astype(BF)
        full = total + lc
        end = full[length - 1 :, :]
        update = (keys * jnp.exp(end - full)).astype(BF)
        states[d] = lax.dot_general(value, update, TN, preferred_element_type=F32)
        sdecay[d] = jnp.broadcast_to(jnp.exp(end), (8, wide))

    def many(body, first, last):
        def one(d, carry):
            body(d)
            return carry

        lax.fori_loop(first, last, one, 0)

    for load in loads[4:]:
        load.wait()
    twin_arrived(0)
    zready(0)
    zready(1)
    project(0, 1, 0, 2)
    twin_arrived(1)
    twin_arrived(2)
    project(1, 2, 0, 2)
    zready(2)
    project(0, 1, 2, 3)
    project(1, 2, 2, 3)
    row_arrived(3, 0)
    row_arrived(3, 1)
    twin(3).start()
    many(local, 0, 3)
    zhop(1, 4)
    zhop(2, 3)
    zhop(2, 4)
    twin_arrived(3)
    project(3, 1, 0, 2)
    project(3, 1, 2, 3)
    many(local, 3, 4)

    out_arrived(2, order(2, 0))
    relay_out(2, 1).start()
    out_arrived(1, order(1, 0))
    relay_out(1, 2).start()

    def state_copy(d):
        return remote(sout.at[d], sin.at[d], ss.at[0], sr.at[d], sp=s + 1)

    def place(j, g):
        return mix.at[:, pl.ds(pl.multiple_of(j * depth + g * wide, wide), wide)]

    def mixed_send(d, j):
        return remote(msend.at[d - 1, j], place(j, f), xs.at[0], xr.at[0], fs=f ^ d)

    def deliver(d, j, value):
        if d == 0:
            mix[:, pl.ds(pl.multiple_of(j * depth + f * wide, wide), wide)] = value
        else:
            msend[d - 1, j] = value
            mixed_send(d, j).start()

    def chain(d):
        @pl.when(has_left)
        def _():
            state_copy(d).wait_recv()

        @pl.when(s == 0)
        def _():
            sin[d] = jnp.zeros(sin.shape[1:], BF)

        @pl.when(has_right)
        def _():
            sout[d] = (sin[d].astype(F32) * sdecay[d, 0:1, :] + states[d]).astype(BF)
            state_copy(d).start()

        raw = inside[d] + lax.dot_general(reach[d], sin[d], NT, preferred_element_type=F32)
        scale = lax.rsqrt(jnp.mean(raw * raw, axis=-1, keepdims=True) + 1e-06)
        deliver(d, 1, (raw * scale * hgain[...]).astype(BF))

    turns = (3, 1, 2, 0)
    last = s == ns - 1
    inland = jnp.logical_not(last)


    edge = rim.shape[1]

    def rim_copy():
        return remote(brim, rim, ms.at[0], mr.at[0], sp=s + 1)

    def swaps(side):
        for core in range(2):
            @pl.when(t == core)
            def _(core=core):
                for d in (1, 2):
                    swap(d, side, core).start()

    def signal():
        zready(3)

        @pl.when(has_right)
        def _():
            ends_ = rows[:, pl.ds(length - edge, edge), :].reshape(nf * edge, rows.shape[2])
            made = jnp.dot(ends_, wg[:, pl.ds(SIGNAL * wide, wide)], preferred_element_type=F32).astype(BF)
            brim[...] = made.reshape(nf, edge, wide)
            rim_copy().start()

        @pl.when(s == 0)
        def _():
            rim[...] = jnp.zeros(rim.shape, BF)

        @pl.when((odd == 0) & (s > 0))
        def _():
            swaps(0)

        def one(d, carry):
            project(d, 1, 3, 4)
            return carry

        lax.fori_loop(0, nf, one, 0)

    def assists():
        for i in range(2):
            out_arrived(3, 2 * odd + i)
            assist(i).start()

    @pl.when(odd == 1)
    def _():
        swaps(1)

    def thirds():
        for to_d in (1, 2):
            third_upper(to_d).start()

    @pl.when(last)
    def _():
        thirds()
        signal()
        assists()

    for d in turns:
        chain(d)

    @pl.when(s == 0)
    def _():
        swaps(0)

    @pl.when(inland)
    def _():
        thirds()
        signal()

    @pl.when(inland)
    def _():
        assists()


    @pl.when(has_left)
    def _():
        rim_copy().wait_recv()

    def filtering(d):
        padded = jnp.concatenate([rim[d], group(d, SIGNAL)], axis=0).astype(F32)
        margin = taps.shape[1] - 1
        filtered = jnp.zeros((length, wide), F32)
        for o in range(margin + 1):
            start = edge - margin + o
            filtered = filtered + taps[f, o : o + 1, :] * padded[start : start + length]
        filt[d] = filtered

    many(filtering, 0, nf)
    zready(4)
    for d in turns:
        project(d, 1, 4, 5)
        deliver(d, 0, (group(d, GATE).astype(F32) * filt[d]).astype(BF))
    for to_d in (1, 2):
        third_lower(to_d).start()

    def fourths(side, core):
        for to_d in (1, 2):
            fourth(to_d, side, core).start()

    by_side(fourths)


    mixed = remote(msend, msend, xs.at[0], xr.at[0], fs=f ^ 1)
    mixed.wait_recv()

    def rows_of(core):
        return pl.ds(pl.multiple_of(core * half, half), half)

    def finish(chunks):
        spans = []
        for d, c in chunks:
            co = pl.ds(pl.multiple_of(c * 2 * pw, 2 * pw), 2 * pw)
            at = pl.ds(pl.multiple_of((f ^ d) * cols + c * 2 * pw, 2 * pw), 2 * pw)
            shares[:, at] = jnp.dot(mix[...], wo[d, :, co], preferred_element_type=F32).astype(BF)
            spans.append(at)
        for at in spans:
            remote(shares.at[rows_of(other), at], twin_part.at[0, :, at], es.at[0], er.at[0], tp=other).start()
        for at in spans:
            pltpu.make_async_copy(shares.at[rows_of(t), at], part.at[0, :, at], fin.at[0]).start()

    def last_quarters(d):
        third_upper(d).wait_recv()
        out_arrived(d, order(d, 2), lower)

        def rest(side, core):
            swapped(d, side, core)
            out_arrived(d, order(d, 3), (taken(side, core), 2 * depth - taken(side, core)))

        by_side(rest)

    def assisted(d):
        for q in (2 - 2 * odd, 3 - 2 * odd):
            out_arrived(3, q)

    for d in (1, 2):
        out_arrived(d, order(d, 1))
    finish([(0, odd), (0, 1 - odd), (1, odd), (2, odd), (3, odd)])
    for d in (1, 2):
        last_quarters(d)
    assisted(3)
    finish([(1, 1 - odd), (2, 1 - odd), (3, 1 - odd)])


    def drained(ref, sem):
        pltpu.make_async_copy(ref, ref, sem).wait()

    @pl.when(inner)
    def _():
        drained(wg, zs.at[0])

    own_rows = wg.at[pl.ds(pl.multiple_of(s * kd, kd), kd), :]

    @pl.when(s == 0)
    def _():
        drained(own_rows, zs.at[0])

    @pl.when(has_left)
    def _():
        drained(own_rows, zsl.at[0])

    drained(rows.at[pl.ds(0, 3), pl.ds(0, half), :], rs.at[0])
    drained(rows.at[:, pl.ds(0, half), :], ts.at[0])
    drained(others, ls.at[0])
    drained(msend, xs.at[0])

    def quarters(side, core):
        count = 2 * (8 * depth - taken(side, core)) + 8 * depth + 2 * taken(1 - side, core)
        drained(wo.at[:, pl.ds(0, count // 16), :], os_.at[0])

    by_side(quarters)

    @pl.when(has_right)
    def _():
        drained(sout, ss.at[0])
        drained(brim, ms.at[0])

    mine = shares.at[rows_of(t), :]
    drained(mine, es.at[0])
    drained(mine, fin.at[0])
    drained(mine, er.at[0])


def body(ns, nf, tokens, norm_gain, w0, w1, w2, w3, w4, conv_taps, floor_gate, leak, head_gain, cow, how):
    half, width = tokens.shape[1:]
    length = 2 * half
    heads = leak.shape[2]
    kd = w0.shape[0]
    wide = w0.shape[1] // nf
    assert heads == nf and nf == 4 and floor_gate.shape[0] == heads * wide and ns % 2 == 0
    taps = conv_taps.reshape(conv_taps.shape[0], nf, wide).transpose(1, 0, 2)
    hbm = pl.BlockSpec(memory_space=pltpu.HBM)
    dma = pltpu.SemaphoreType.DMA
    depth, cols = cow.shape
    scratch = [
        pltpu.VMEM((half, width), BF),
        pltpu.VMEM((1, width), F32),
        pltpu.VMEM(taps.shape, F32),
        pltpu.VMEM((heads, 1, wide), F32),
        pltpu.VMEM((heads, length), F32),
        pltpu.VMEM((1, wide), F32),
        pltpu.VMEM((nf, length, width), BF),
        pltpu.VMEM((ns * kd, 5 * wide), BF),
        pltpu.VMEM((nf, length, 5 * wide), BF),
        pltpu.VMEM((nf, 2 * depth, cols), BF),
        pltpu.VMEM((nf, 16, wide), BF),
        pltpu.VMEM((nf, 16, wide), BF),
        pltpu.VMEM((nf, length, wide), F32),
        pltpu.VMEM((nf, length, wide), F32),
        pltpu.VMEM((nf, length, wide), BF),
        pltpu.VMEM((nf, wide, wide), F32),
        pltpu.VMEM((nf, 8, wide), F32),
        pltpu.VMEM((nf, wide, wide), BF),
        pltpu.VMEM((nf, wide, wide), BF),
        pltpu.VMEM((nf, 8, length), F32),
        pltpu.VMEM((nf, length, wide), F32),
        pltpu.VMEM((nf, 8, length), F32),
        pltpu.VMEM((nf - 1, 2, length, wide), BF),
        pltpu.VMEM((length, 2 * depth), BF),
        pltpu.VMEM((length, width), BF),
        dma((7,)), dma((1,)), dma((1,)), dma((ns, 5)), dma((5,)),
        dma((1,)), dma((nf - 1, 2)), dma((1,)), dma((nf,)), dma((1,)), dma((1,)),
        dma((1,)), dma((1,)), dma((3, 4)), dma((2,)), dma((2,)),
        dma((1,)), dma((1,)), dma((1,)), dma((1,)), dma((1,)), dma((nf,)),
        dma((1,)), dma((1,)), dma((1,)),
    ]
    part, twin_part = pl.pallas_call(
        functools.partial(kernel, ns, nf),
        out_shape=[jax.ShapeDtypeStruct(tokens.shape, BF)] * 2,
        in_specs=[hbm] * 13,
        out_specs=[hbm] * 2,
        scratch_shapes=scratch,
        compiler_params=pltpu.CompilerParams(
            collective_id=0, has_side_effects=True, vmem_limit_bytes=60 * 2**20
        ),
    )(
        tokens, norm_gain[None], w0, w1, w2, w3, w4, taps, floor_gate.reshape(heads, 1, wide),
        leak[0].T, head_gain[None], cow, how,
    )
    return (part.astype(F32) + twin_part.astype(F32)).astype(BF)


def solution(mesh):
    in_specs = (
        P("fs", ("sp", "tp"), None),
        P(),
        P("sp", "tp"),
        P("sp", "tp"),
        P("sp", "tp"),
        P("sp", "tp"),
        P("sp", "tp"),
        P(None, "tp"),
        P("tp"),
        P("fs", "sp", "tp"),
        P(),
        P("tp", "fs"),
        P("tp", "fs"),
    )
    out_specs = P("fs", ("sp", "tp"), None)
    step = functools.partial(body, mesh.shape["sp"], mesh.shape["fs"])
    return jax.shard_map(step, mesh=mesh, in_specs=in_specs, out_specs=out_specs, check_vma=False)
```

```python
import functools

import jax
import jax.numpy as jnp
from jax import lax
from jax.experimental import pallas as pl
from jax.experimental.pallas import tpu as pltpu
from jax.sharding import PartitionSpec as P

MESH = pl.DeviceIdType.MESH
BF = jnp.bfloat16
F32 = jnp.float32
NT = (((1,), (1,)), ((), ()))
TN = (((0,), (0,)), ((), ()))
GATE, SIGNAL, QUERY, FORGET, VALUE = 4, 3, 1, 0, 2


def kernel(
    ns, nf,
    tok_h, gain_h, w0, w1, w2, w3, w4, taps_h, floor_h, leak_h, hgain_h, cow, how,
    part, twin_part,
    tokv, gain, taps, floor, leak_t, hgain,
    rows, wg, y, wo, brim, rim, filt, inside, reach, states, sdecay, sin, sout,
    lk, lcol, lrow, msend, mix, shares,
    il, zs, zsl, zr, zloc, rs, rr, ts, tr, ls, lr, oloc, os_, or_, ov, zc, xs, xr, ms, mr, ss, sr, es, er, fin,
):
    s, f, t = lax.axis_index("sp"), lax.axis_index("fs"), lax.axis_index("tp")
    other = 1 - t
    half = tokv.shape[0]
    length = 2 * half
    kd = w0.shape[0]
    wide = w0.shape[1] // nf
    ws = (w3, w2, w4, w1, w0)
    np_ = len(ws)
    has_left, has_right = s > 0, s < ns - 1
    inner = has_left & has_right
    outs = (cow, how)
    depth, cols = cow.shape
    odd = lax.rem(s, 2)
    mate = s + 1 - 2 * odd

    def remote(src, dst, send, recv, **where):
        return pltpu.make_async_remote_copy(
            src_ref=src, dst_ref=dst, send_sem=send, recv_sem=recv,
            device_id=where, device_id_type=MESH,
        )


    def wblock(b, p):
        return wg.at[pl.ds(pl.multiple_of(b * kd, kd), kd), pl.ds(p * wide, wide)]

    def wload(p):
        return pltpu.make_async_copy(
            ws[p].at[:, pl.ds(pl.multiple_of(f * wide, wide), wide)], wblock(s, p), zloc.at[p]
        )

    def oload(j):
        return pltpu.make_async_copy(outs[j], wo.at[0, pl.ds(j * depth, depth), :], oloc.at[0])

    quarter = half // 2
    pieces = [pl.ds(j * quarter, quarter) for j in range(2)]
    loads = [
        pltpu.make_async_copy(src, dst, il.at[i])
        for i, (src, dst) in enumerate(
            (
                (tok_h.at[0, pieces[0]], tokv.at[pieces[0]]), (gain_h, gain), (tok_h.at[0, pieces[1]], tokv.at[pieces[1]]),
                (leak_h, leak_t), (taps_h, taps), (floor_h, floor), (hgain_h, hgain),
            )
        )
    ]

    barrier = pltpu.get_barrier_semaphore()
    for d in range(nf - 1, 0, -1):
        pl.semaphore_signal(barrier, inc=1, device_id={"fs": f ^ d}, device_id_type=MESH)

    @pl.when(has_left)
    def _():
        pl.semaphore_signal(barrier, inc=1, device_id={"sp": s - 1}, device_id_type=MESH)

    @pl.when(has_right)
    def _():
        pl.semaphore_signal(barrier, inc=1, device_id={"sp": s + 1}, device_id_type=MESH)

    pl.semaphore_signal(barrier, inc=1, device_id={"tp": other}, device_id_type=MESH)

    for load in loads[:4]:
        load.start()
    wload(0).start()
    wload(1).start()
    for load in loads[4:]:
        load.start()
    for p in range(2, np_):
        wload(p).start()
    for j in range(2):
        oload(j).start()


    loads[3].wait()
    lk[0, pl.ds(0, leak_t.shape[0]), :] = leak_t[...]

    def normalize(j):
        for load in loads[2 * j : 2 + j]:
            load.wait()
        x = tokv[pieces[j]].astype(F32)
        center = x - jnp.mean(x, axis=-1, keepdims=True)
        spread = jnp.mean(center * center, axis=-1, keepdims=True)
        rows[0, pl.ds(pl.multiple_of(t * half + j * quarter, quarter), quarter), :] = (
            center * lax.rsqrt(spread + 1e-05) * gain[...]
        ).astype(BF)

    normalize(0)
    ends = jnp.where(has_left, 1, 0) + jnp.where(has_right, 1, 0)
    pl.semaphore_wait(barrier, nf + ends)


    def own_right(p):
        return remote(wblock(s, p), wblock(s, p), zs.at[0], zr.at[s, p], sp=s + 1)

    def own_left(p):
        return remote(wblock(s, p), wblock(s, p), zsl.at[0], zr.at[s, p], sp=s - 1)

    def relay(b, p, to):
        return remote(wblock(b, p), wblock(b, p), zs.at[0], zr.at[b, p], sp=to)

    def send_own(p, where):
        @pl.when(where & has_right)
        def _():
            own_right(p).start()

        @pl.when(where & has_left)
        def _():
            own_left(p).start()

    def zhop(k, p):
        @pl.when((s - k >= 0) & has_right)
        def _():
            relay(s - k, p, s + 1).wait_recv()
            relay(s - k, p, s + 1).start()

        @pl.when((s + k < ns) & has_left)
        def _():
            relay(s + k, p, s - 1).wait_recv()
            relay(s + k, p, s - 1).start()

    def zready(p):
        def far(k, carry):
            zhop(k, p)
            return carry

        if ns > 3:
            lax.fori_loop(3, ns, far, 0)

        def hop(k, carry):
            @pl.when((s - k >= 0) & (s == ns - 1))
            def _():
                relay(s - k, p, s - 1).wait_recv()

            @pl.when((s + k < ns) & (s == 0))
            def _():
                relay(s + k, p, s + 1).wait_recv()

            return carry

        lax.fori_loop(1, ns, hop, 0)

    always = s >= 0
    for p in range(2):
        wload(p).wait()
        send_own(p, always)

    def piece(d, j):
        return rows.at[d, pl.ds(pl.multiple_of(t * half + j * quarter, quarter), quarter), :]

    def core_rows(d, core):
        return rows.at[d, pl.ds(pl.multiple_of(core * half, half), half), :]

    def row_send(d, j, to_d):
        return remote(piece(d, j), piece(d ^ to_d, j), rs.at[0], rr.at[(d ^ to_d) - 1, j], fs=f ^ to_d)

    def row_arrived(d, j):
        remote(piece(d, j), piece(d, j), rs.at[0], rr.at[d - 1, j], fs=f ^ 1).wait_recv()

    def twin(d):
        return remote(core_rows(d, t), core_rows(d, t), ts.at[0], tr.at[d], tp=other)

    def twin_arrived(d):
        remote(core_rows(d, other), core_rows(d, other), ts.at[0], tr.at[d], tp=other).wait_recv()

    def leak_send(d):
        return remote(lk.at[0], lk.at[d], ls.at[0], lr.at[0], fs=f ^ d)

    for d in range(1, nf):
        leak_send(d).start()
    row_send(0, 0, 1).start()
    normalize(1)
    row_send(0, 1, 2).start()
    row_send(0, 1, 1).start()
    row_send(0, 0, 2).start()
    twin(0).start()
    for p in range(2, np_):
        wload(p).wait()
        send_own(p, jnp.logical_not(inner))

    zhop(1, 0)
    zhop(1, 1)


    others = lk.at[pl.ds(1, nf - 1)]
    remote(others, others, ls.at[0], lr.at[0], fs=f ^ 1).wait_recv()
    ri = lax.broadcasted_iota(jnp.int32, (length, length), 0)
    ci = lax.broadcasted_iota(jnp.int32, (length, length), 1)
    tril = (ri >= ci).astype(F32)
    triu = (ri <= ci).astype(F32)
    high = lax.Precision.HIGHEST
    head_leak = jnp.concatenate(
        [lk[d, pl.ds(f, 1), :] for d in range(nf)] + [jnp.zeros((8 - nf, length), F32)], axis=0
    )
    lsum = lax.dot_general(tril, head_leak, NT, precision=high, preferred_element_type=F32)
    lsum_t = jnp.dot(head_leak, triu, precision=high, preferred_element_type=F32)
    for d in range(nf):
        lcol[d] = jnp.broadcast_to(lsum[:, d : d + 1], (length, wide))
        lrow[d] = jnp.broadcast_to(lsum_t[d : d + 1, :], (8, length))

    zhop(2, 0)
    send_own(2, inner)


    pw = cols // 4

    full = (0, 2 * depth)

    def opiece(d, q, part=full):
        return wo.at[d, pl.ds(*part), pl.ds(pl.multiple_of(q * pw, pw), pw)]

    def order(to_d, i):
        low, high = 2 * odd, 2 - 2 * odd
        return ((low + 1, low, high, high + 1) if to_d == 1 else (low, low + 1, high + 1, high))[i]

    lower, upper = (0, depth), (depth, depth)

    def own_out(to_d, i, part=full):
        q = order(to_d, i)
        return remote(opiece(0, q, part), opiece(to_d, q, part), os_.at[0], or_.at[to_d - 1, q], fs=f ^ to_d)

    def out_arrived(d, q, part=full):
        remote(opiece(d, q, part), opiece(d, q, part), os_.at[0], or_.at[d - 1, q], fs=f ^ 1).wait_recv()

    def third_upper(to_d):
        q = order(to_d, 2)
        return remote(opiece(0, q, upper), opiece(to_d, q, upper), os_.at[0], ov.at[to_d - 1], fs=f ^ to_d)

    def third_lower(to_d):
        return own_out(to_d, 2, lower)

    def taken(side, core):
        return depth * ((6, 4), (2, 1))[core][side] // 4

    def fourth(to_d, side, core):
        return own_out(to_d, 3, (taken(side, core), 2 * depth - taken(side, core)))

    def swap(d, side, core):
        q, part = order(d, 0), (0, taken(1 - side, core))
        return remote(opiece(d, q, part), opiece(d, q, part), os_.at[0], zc.at[d - 1], sp=mate)

    def swapped(d, side, core):
        q, part = order(d, 3), (0, taken(side, core))
        remote(opiece(d, q, part), opiece(d, q, part), os_.at[0], zc.at[d - 1], sp=mate).wait_recv()

    def by_side(work):
        for side in range(2):
            for core in range(2):
                @pl.when((odd == side) & (t == core))
                def _(side=side, core=core):
                    work(side, core)

    def relay_out(d, to_d):
        q = order(d, 0)
        return remote(opiece(d, q), opiece(3, q), os_.at[0], or_.at[2, q], fs=f ^ to_d)

    def assist(i):
        q = 2 * odd + i
        return remote(opiece(3, q), opiece(3, q), os_.at[0], or_.at[2, q], sp=mate)

    row_arrived(1, 0)
    row_send(1, 0, 2).start()
    row_arrived(2, 1)
    row_send(2, 1, 1).start()
    pltpu.make_async_copy(wo.at[0], wo.at[0], oloc.at[0]).wait()
    for i in range(2):
        own_out(1, i).start()
        own_out(2, i).start()

    zhop(1, 2)
    zhop(2, 1)
    zhop(2, 2)
    send_own(3, inner)
    row_arrived(1, 1)
    twin(1).start()
    row_arrived(2, 0)
    twin(2).start()
    zhop(1, 3)
    send_own(4, inner)

    def project(d, n, p, q):
        left = rows[pl.ds(d, n)].reshape(n * length, rows.shape[2])
        co = pl.ds(p * wide, (q - p) * wide)
        made = jnp.dot(left, wg[:, co], preferred_element_type=F32).astype(BF)
        y[pl.ds(d, n), :, co] = made.reshape(n, length, (q - p) * wide)

    def group(d, p):
        return y[d, :, p * wide : (p + 1) * wide]

    causal = ri >= ci
    tril_short = tril.astype(BF)

    def local(d):
        fl = floor[f]
        logits = group(d, FORGET).astype(F32)
        retain = fl + (1.0 - fl) * jax.nn.sigmoid(logits)
        keys = (1.0 - fl) * jax.nn.sigmoid(-logits)
        step = jnp.log(retain)
        coarse = step.astype(BF)
        fine = (step - coarse.astype(F32)).astype(BF)
        both = jnp.dot(
            tril_short, jnp.concatenate([coarse, fine], axis=1), preferred_element_type=F32
        )
        total = both[:, :wide] + both[:, wide:]
        raw = group(d, QUERY).astype(F32)
        query = raw * jax.nn.sigmoid(raw) * jnp.exp(total)
        value = group(d, VALUE)
        scores = lax.dot_general(
            query.astype(BF), (keys * jnp.exp(-total)).astype(BF), NT, preferred_element_type=F32
        )
        lc = lcol[d]
        gap = lc[:, 0:1] - lrow[d, 0:1, :]
        scores = jnp.where(causal, scores * jnp.exp(jnp.where(causal, gap, 0.0)), 0.0)
        inside[d] = jnp.dot(scores.astype(BF), value, preferred_element_type=F32)
        reach[d] = (query * jnp.exp(lc)).astype(BF)
        full = total + lc
        end = full[length - 1 :, :]
        update = (keys * jnp.exp(end - full)).astype(BF)
        states[d] = lax.dot_general(value, update, TN, preferred_element_type=F32)
        sdecay[d] = jnp.broadcast_to(jnp.exp(end), (8, wide))

    def many(body, first, last):
        def one(d, carry):
            body(d)
            return carry

        lax.fori_loop(first, last, one, 0)

    for load in loads[4:]:
        load.wait()
    twin_arrived(0)
    zready(0)
    zready(1)
    project(0, 1, 0, 2)
    twin_arrived(1)
    twin_arrived(2)
    project(1, 2, 0, 2)
    zready(2)
    project(0, 1, 2, 3)
    project(1, 2, 2, 3)
    row_arrived(3, 0)
    row_arrived(3, 1)
    twin(3).start()
    many(local, 0, 3)
    zhop(2, 3)
    zhop(1, 4)
    zhop(2, 4)
    twin_arrived(3)
    project(3, 1, 0, 2)
    project(3, 1, 2, 3)
    many(local, 3, 4)

    out_arrived(2, order(2, 0))
    relay_out(2, 1).start()
    out_arrived(1, order(1, 0))
    relay_out(1, 2).start()

    def state_copy(d):
        return remote(sout.at[d], sin.at[d], ss.at[0], sr.at[d], sp=s + 1)

    def place(j, g):
        return mix.at[:, pl.ds(pl.multiple_of(j * depth + g * wide, wide), wide)]

    def mixed_send(d, j):
        return remote(msend.at[d - 1, j], place(j, f), xs.at[0], xr.at[0], fs=f ^ d)

    def deliver(d, j, value):
        if d == 0:
            mix[:, pl.ds(pl.multiple_of(j * depth + f * wide, wide), wide)] = value
        else:
            msend[d - 1, j] = value
            mixed_send(d, j).start()

    def chain(d):
        @pl.when(has_left)
        def _():
            state_copy(d).wait_recv()

        @pl.when(s == 0)
        def _():
            sin[d] = jnp.zeros(sin.shape[1:], BF)

        @pl.when(has_right)
        def _():
            sout[d] = (sin[d].astype(F32) * sdecay[d, 0:1, :] + states[d]).astype(BF)
            state_copy(d).start()

        raw = inside[d] + lax.dot_general(reach[d], sin[d], NT, preferred_element_type=F32)
        scale = lax.rsqrt(jnp.mean(raw * raw, axis=-1, keepdims=True) + 1e-06)
        deliver(d, 1, (raw * scale * hgain[...]).astype(BF))

    turns = (3, 1, 2, 0)
    last = s == ns - 1
    inland = jnp.logical_not(last)


    edge = rim.shape[1]

    def rim_copy():
        return remote(brim, rim, ms.at[0], mr.at[0], sp=s + 1)

    def swaps(side):
        for core in range(2):
            @pl.when(t == core)
            def _(core=core):
                for d in (1, 2):
                    swap(d, side, core).start()

    def signal():
        zready(3)

        @pl.when(has_right)
        def _():
            ends_ = rows[:, pl.ds(length - edge, edge), :].reshape(nf * edge, rows.shape[2])
            made = jnp.dot(ends_, wg[:, pl.ds(SIGNAL * wide, wide)], preferred_element_type=F32).astype(BF)
            brim[...] = made.reshape(nf, edge, wide)
            rim_copy().start()

        @pl.when(s == 0)
        def _():
            rim[...] = jnp.zeros(rim.shape, BF)

        @pl.when((odd == 0) & (s > 0))
        def _():
            swaps(0)

        def one(d, carry):
            project(d, 1, 3, 4)
            return carry

        lax.fori_loop(0, nf, one, 0)

    def assists():
        for i in range(2):
            out_arrived(3, 2 * odd + i)
            assist(i).start()

    @pl.when(odd == 1)
    def _():
        swaps(1)

    def thirds():
        for to_d in (1, 2):
            third_upper(to_d).start()

    @pl.when(last)
    def _():
        thirds()
        signal()
        assists()

    for d in turns:
        chain(d)

    @pl.when(s == 0)
    def _():
        swaps(0)

    @pl.when(inland)
    def _():
        thirds()
        signal()

    @pl.when(inland)
    def _():
        assists()


    @pl.when(has_left)
    def _():
        rim_copy().wait_recv()

    def filtering(d):
        padded = jnp.concatenate([rim[d], group(d, SIGNAL)], axis=0).astype(F32)
        margin = taps.shape[1] - 1
        filtered = jnp.zeros((length, wide), F32)
        for o in range(margin + 1):
            start = edge - margin + o
            filtered = filtered + taps[f, o : o + 1, :] * padded[start : start + length]
        filt[d] = filtered

    many(filtering, 0, nf)
    zready(4)
    for d in turns:
        project(d, 1, 4, 5)
        deliver(d, 0, (group(d, GATE).astype(F32) * filt[d]).astype(BF))
    for to_d in (1, 2):
        third_lower(to_d).start()

    def fourths(side, core):
        for to_d in (1, 2):
            fourth(to_d, side, core).start()

    by_side(fourths)


    mixed = remote(msend, msend, xs.at[0], xr.at[0], fs=f ^ 1)
    mixed.wait_recv()

    def rows_of(core):
        return pl.ds(pl.multiple_of(core * half, half), half)

    def finish(chunks):
        spans = []
        for d, c in chunks:
            co = pl.ds(pl.multiple_of(c * 2 * pw, 2 * pw), 2 * pw)
            at = pl.ds(pl.multiple_of((f ^ d) * cols + c * 2 * pw, 2 * pw), 2 * pw)
            shares[:, at] = jnp.dot(mix[...], wo[d, :, co], preferred_element_type=F32).astype(BF)
            spans.append(at)
        for at in spans:
            remote(shares.at[rows_of(other), at], twin_part.at[0, :, at], es.at[0], er.at[0], tp=other).start()
        for at in spans:
            pltpu.make_async_copy(shares.at[rows_of(t), at], part.at[0, :, at], fin.at[0]).start()

    def last_quarters(d):
        third_upper(d).wait_recv()
        out_arrived(d, order(d, 2), lower)

        def rest(side, core):
            swapped(d, side, core)
            out_arrived(d, order(d, 3), (taken(side, core), 2 * depth - taken(side, core)))

        by_side(rest)

    def assisted(d):
        for q in (2 - 2 * odd, 3 - 2 * odd):
            out_arrived(3, q)

    for d in (1, 2):
        out_arrived(d, order(d, 1))
    finish([(0, odd), (0, 1 - odd), (1, odd), (2, odd), (3, odd)])
    for d in (1, 2):
        last_quarters(d)
    assisted(3)
    finish([(1, 1 - odd), (2, 1 - odd), (3, 1 - odd)])


    def drained(ref, sem):
        pltpu.make_async_copy(ref, ref, sem).wait()

    @pl.when(inner)
    def _():
        drained(wg, zs.at[0])

    own_rows = wg.at[pl.ds(pl.multiple_of(s * kd, kd), kd), :]

    @pl.when(s == 0)
    def _():
        drained(own_rows, zs.at[0])

    @pl.when(has_left)
    def _():
        drained(own_rows, zsl.at[0])

    drained(rows.at[pl.ds(0, 3), pl.ds(0, half), :], rs.at[0])
    drained(rows.at[:, pl.ds(0, half), :], ts.at[0])
    drained(others, ls.at[0])
    drained(msend, xs.at[0])

    def quarters(side, core):
        count = 2 * (8 * depth - taken(side, core)) + 8 * depth + 2 * taken(1 - side, core)
        drained(wo.at[:, pl.ds(0, count // 16), :], os_.at[0])

    by_side(quarters)

    @pl.when(has_right)
    def _():
        drained(sout, ss.at[0])
        drained(brim, ms.at[0])

    mine = shares.at[rows_of(t), :]
    drained(mine, es.at[0])
    drained(mine, fin.at[0])
    drained(mine, er.at[0])


def body(ns, nf, tokens, norm_gain, w0, w1, w2, w3, w4, conv_taps, floor_gate, leak, head_gain, cow, how):
    half, width = tokens.shape[1:]
    length = 2 * half
    heads = leak.shape[2]
    kd = w0.shape[0]
    wide = w0.shape[1] // nf
    assert heads == nf and nf == 4 and floor_gate.shape[0] == heads * wide and ns % 2 == 0
    taps = conv_taps.reshape(conv_taps.shape[0], nf, wide).transpose(1, 0, 2)
    hbm = pl.BlockSpec(memory_space=pltpu.HBM)
    dma = pltpu.SemaphoreType.DMA
    depth, cols = cow.shape
    scratch = [
        pltpu.VMEM((half, width), BF),
        pltpu.VMEM((1, width), F32),
        pltpu.VMEM(taps.shape, F32),
        pltpu.VMEM((heads, 1, wide), F32),
        pltpu.VMEM((heads, length), F32),
        pltpu.VMEM((1, wide), F32),
        pltpu.VMEM((nf, length, width), BF),
        pltpu.VMEM((ns * kd, 5 * wide), BF),
        pltpu.VMEM((nf, length, 5 * wide), BF),
        pltpu.VMEM((nf, 2 * depth, cols), BF),
        pltpu.VMEM((nf, 16, wide), BF),
        pltpu.VMEM((nf, 16, wide), BF),
        pltpu.VMEM((nf, length, wide), F32),
        pltpu.VMEM((nf, length, wide), F32),
        pltpu.VMEM((nf, length, wide), BF),
        pltpu.VMEM((nf, wide, wide), F32),
        pltpu.VMEM((nf, 8, wide), F32),
        pltpu.VMEM((nf, wide, wide), BF),
        pltpu.VMEM((nf, wide, wide), BF),
        pltpu.VMEM((nf, 8, length), F32),
        pltpu.VMEM((nf, length, wide), F32),
        pltpu.VMEM((nf, 8, length), F32),
        pltpu.VMEM((nf - 1, 2, length, wide), BF),
        pltpu.VMEM((length, 2 * depth), BF),
        pltpu.VMEM((length, width), BF),
        dma((7,)), dma((1,)), dma((1,)), dma((ns, 5)), dma((5,)),
        dma((1,)), dma((nf - 1, 2)), dma((1,)), dma((nf,)), dma((1,)), dma((1,)),
        dma((1,)), dma((1,)), dma((3, 4)), dma((2,)), dma((2,)),
        dma((1,)), dma((1,)), dma((1,)), dma((1,)), dma((1,)), dma((nf,)),
        dma((1,)), dma((1,)), dma((1,)),
    ]
    part, twin_part = pl.pallas_call(
        functools.partial(kernel, ns, nf),
        out_shape=[jax.ShapeDtypeStruct(tokens.shape, BF)] * 2,
        in_specs=[hbm] * 13,
        out_specs=[hbm] * 2,
        scratch_shapes=scratch,
        compiler_params=pltpu.CompilerParams(
            collective_id=0, has_side_effects=True, vmem_limit_bytes=60 * 2**20
        ),
    )(
        tokens, norm_gain[None], w0, w1, w2, w3, w4, taps, floor_gate.reshape(heads, 1, wide),
        leak[0].T, head_gain[None], cow, how,
    )
    return (part.astype(F32) + twin_part.astype(F32)).astype(BF)


def solution(mesh):
    in_specs = (
        P("fs", ("sp", "tp"), None),
        P(),
        P("sp", "tp"),
        P("sp", "tp"),
        P("sp", "tp"),
        P("sp", "tp"),
        P("sp", "tp"),
        P(None, "tp"),
        P("tp"),
        P("fs", "sp", "tp"),
        P(),
        P("tp", "fs"),
        P("tp", "fs"),
    )
    out_specs = P("fs", ("sp", "tp"), None)
    step = functools.partial(body, mesh.shape["sp"], mesh.shape["fs"])
    return jax.shard_map(step, mesh=mesh, in_specs=in_specs, out_specs=out_specs, check_vma=False)
```

```python
import functools

import jax
import jax.numpy as jnp
from jax import lax
from jax.experimental import pallas as pl
from jax.experimental.pallas import tpu as pltpu
from jax.sharding import PartitionSpec as P

MESH = pl.DeviceIdType.MESH
BF = jnp.bfloat16
F32 = jnp.float32
NT = (((1,), (1,)), ((), ()))
TN = (((0,), (0,)), ((), ()))
GATE, SIGNAL, QUERY, FORGET, VALUE = 4, 3, 1, 0, 2


def kernel(
    ns, nf,
    tok_h, gain_h, w0, w1, w2, w3, w4, taps_h, floor_h, leak_h, hgain_h, cow, how,
    part, twin_part,
    tokv, gain, taps, floor, leak_t, hgain,
    rows, wg, y, wo, brim, rim, filt, inside, reach, states, sdecay, sin, sout,
    lk, lcol, lrow, msend, mix, shares,
    il, zs, zsl, zr, zloc, rs, rr, ts, tr, ls, lr, oloc, os_, or_, ov, zc, xs, xr, ms, mr, ss, sr, es, er, fin,
):
    s, f, t = lax.axis_index("sp"), lax.axis_index("fs"), lax.axis_index("tp")
    other = 1 - t
    half = tokv.shape[0]
    length = 2 * half
    kd = w0.shape[0]
    wide = w0.shape[1] // nf
    ws = (w3, w2, w4, w1, w0)
    np_ = len(ws)
    has_left, has_right = s > 0, s < ns - 1
    inner = has_left & has_right
    outs = (cow, how)
    depth, cols = cow.shape
    odd = lax.rem(s, 2)
    mate = s + 1 - 2 * odd

    def remote(src, dst, send, recv, **where):
        return pltpu.make_async_remote_copy(
            src_ref=src, dst_ref=dst, send_sem=send, recv_sem=recv,
            device_id=where, device_id_type=MESH,
        )


    def wblock(b, p):
        return wg.at[pl.ds(pl.multiple_of(b * kd, kd), kd), pl.ds(p * wide, wide)]

    def wload(p):
        return pltpu.make_async_copy(
            ws[p].at[:, pl.ds(pl.multiple_of(f * wide, wide), wide)], wblock(s, p), zloc.at[p]
        )

    def oload(j):
        return pltpu.make_async_copy(outs[j], wo.at[0, pl.ds(j * depth, depth), :], oloc.at[0])

    quarter = half // 2
    pieces = [pl.ds(j * quarter, quarter) for j in range(2)]
    loads = [
        pltpu.make_async_copy(src, dst, il.at[i])
        for i, (src, dst) in enumerate(
            (
                (tok_h.at[0, pieces[0]], tokv.at[pieces[0]]), (gain_h, gain), (tok_h.at[0, pieces[1]], tokv.at[pieces[1]]),
                (leak_h, leak_t), (taps_h, taps), (floor_h, floor), (hgain_h, hgain),
            )
        )
    ]

    barrier = pltpu.get_barrier_semaphore()
    for d in range(nf - 1, 0, -1):
        pl.semaphore_signal(barrier, inc=1, device_id={"fs": f ^ d}, device_id_type=MESH)

    @pl.when(has_left)
    def _():
        pl.semaphore_signal(barrier, inc=1, device_id={"sp": s - 1}, device_id_type=MESH)

    @pl.when(has_right)
    def _():
        pl.semaphore_signal(barrier, inc=1, device_id={"sp": s + 1}, device_id_type=MESH)

    pl.semaphore_signal(barrier, inc=1, device_id={"tp": other}, device_id_type=MESH)

    for load in loads[:4]:
        load.start()
    wload(0).start()
    wload(1).start()
    for load in loads[4:]:
        load.start()
    for p in range(2, np_):
        wload(p).start()
    for j in range(2):
        oload(j).start()


    loads[3].wait()
    lk[0, pl.ds(0, leak_t.shape[0]), :] = leak_t[...]

    def normalize(j):
        for load in loads[2 * j : 2 + j]:
            load.wait()
        x = tokv[pieces[j]].astype(F32)
        center = x - jnp.mean(x, axis=-1, keepdims=True)
        spread = jnp.mean(center * center, axis=-1, keepdims=True)
        rows[0, pl.ds(pl.multiple_of(t * half + j * quarter, quarter), quarter), :] = (
            center * lax.rsqrt(spread + 1e-05) * gain[...]
        ).astype(BF)

    normalize(0)
    ends = jnp.where(has_left, 1, 0) + jnp.where(has_right, 1, 0)
    pl.semaphore_wait(barrier, nf + ends)


    def own_right(p):
        return remote(wblock(s, p), wblock(s, p), zs.at[0], zr.at[s, p], sp=s + 1)

    def own_left(p):
        return remote(wblock(s, p), wblock(s, p), zsl.at[0], zr.at[s, p], sp=s - 1)

    def relay(b, p, to):
        return remote(wblock(b, p), wblock(b, p), zs.at[0], zr.at[b, p], sp=to)

    def send_own(p, where):
        @pl.when(where & has_right)
        def _():
            own_right(p).start()

        @pl.when(where & has_left)
        def _():
            own_left(p).start()

    def zhop(k, p):
        @pl.when((s - k >= 0) & has_right)
        def _():
            relay(s - k, p, s + 1).wait_recv()
            relay(s - k, p, s + 1).start()

        @pl.when((s + k < ns) & has_left)
        def _():
            relay(s + k, p, s - 1).wait_recv()
            relay(s + k, p, s - 1).start()

    def zready(p):
        def far(k, carry):
            zhop(k, p)
            return carry

        if ns > 3:
            lax.fori_loop(3, ns, far, 0)

        def hop(k, carry):
            @pl.when((s - k >= 0) & (s == ns - 1))
            def _():
                relay(s - k, p, s - 1).wait_recv()

            @pl.when((s + k < ns) & (s == 0))
            def _():
                relay(s + k, p, s + 1).wait_recv()

            return carry

        lax.fori_loop(1, ns, hop, 0)

    always = s >= 0
    for p in range(2):
        wload(p).wait()
        send_own(p, always)

    def piece(d, j):
        return rows.at[d, pl.ds(pl.multiple_of(t * half + j * quarter, quarter), quarter), :]

    def core_rows(d, core):
        return rows.at[d, pl.ds(pl.multiple_of(core * half, half), half), :]

    def row_send(d, j, to_d):
        return remote(piece(d, j), piece(d ^ to_d, j), rs.at[0], rr.at[(d ^ to_d) - 1, j], fs=f ^ to_d)

    def row_arrived(d, j):
        remote(piece(d, j), piece(d, j), rs.at[0], rr.at[d - 1, j], fs=f ^ 1).wait_recv()

    def twin(d):
        return remote(core_rows(d, t), core_rows(d, t), ts.at[0], tr.at[d], tp=other)

    def twin_arrived(d):
        remote(core_rows(d, other), core_rows(d, other), ts.at[0], tr.at[d], tp=other).wait_recv()

    def leak_send(d):
        return remote(lk.at[0], lk.at[d], ls.at[0], lr.at[0], fs=f ^ d)

    for d in range(1, nf):
        leak_send(d).start()
    row_send(0, 0, 1).start()
    normalize(1)
    row_send(0, 1, 2).start()
    row_send(0, 1, 1).start()
    row_send(0, 0, 2).start()
    twin(0).start()
    for p in range(2, np_):
        wload(p).wait()
        send_own(p, jnp.logical_not(inner))

    zhop(1, 0)
    zhop(1, 1)


    others = lk.at[pl.ds(1, nf - 1)]
    remote(others, others, ls.at[0], lr.at[0], fs=f ^ 1).wait_recv()
    ri = lax.broadcasted_iota(jnp.int32, (length, length), 0)
    ci = lax.broadcasted_iota(jnp.int32, (length, length), 1)
    tril = (ri >= ci).astype(F32)
    triu = (ri <= ci).astype(F32)
    high = lax.Precision.HIGHEST
    head_leak = jnp.concatenate(
        [lk[d, pl.ds(f, 1), :] for d in range(nf)] + [jnp.zeros((8 - nf, length), F32)], axis=0
    )
    lsum = lax.dot_general(tril, head_leak, NT, precision=high, preferred_element_type=F32)
    lsum_t = jnp.dot(head_leak, triu, precision=high, preferred_element_type=F32)
    for d in range(nf):
        lcol[d] = jnp.broadcast_to(lsum[:, d : d + 1], (length, wide))
        lrow[d] = jnp.broadcast_to(lsum_t[d : d + 1, :], (8, length))

    zhop(2, 0)
    send_own(2, inner)


    pw = cols // 4

    full = (0, 2 * depth)

    def opiece(d, q, part=full):
        return wo.at[d, pl.ds(*part), pl.ds(pl.multiple_of(q * pw, pw), pw)]

    def order(to_d, i):
        low, high = 2 * odd, 2 - 2 * odd
        return ((low + 1, low, high, high + 1) if to_d == 1 else (low, low + 1, high + 1, high))[i]

    lower, upper = (0, depth), (depth, depth)

    def own_out(to_d, i, part=full):
        q = order(to_d, i)
        return remote(opiece(0, q, part), opiece(to_d, q, part), os_.at[0], or_.at[to_d - 1, q], fs=f ^ to_d)

    def out_arrived(d, q, part=full):
        remote(opiece(d, q, part), opiece(d, q, part), os_.at[0], or_.at[d - 1, q], fs=f ^ 1).wait_recv()

    def third_upper(to_d):
        q = order(to_d, 2)
        return remote(opiece(0, q, upper), opiece(to_d, q, upper), os_.at[0], ov.at[to_d - 1], fs=f ^ to_d)

    def third_lower(to_d):
        return own_out(to_d, 2, lower)

    def taken(side, core):
        return depth * ((5, 4), (2, 1))[core][side] // 4

    def fourth(to_d, side, core):
        return own_out(to_d, 3, (taken(side, core), 2 * depth - taken(side, core)))

    def swap(d, side, core):
        q, part = order(d, 0), (0, taken(1 - side, core))
        return remote(opiece(d, q, part), opiece(d, q, part), os_.at[0], zc.at[d - 1], sp=mate)

    def swapped(d, side, core):
        q, part = order(d, 3), (0, taken(side, core))
        remote(opiece(d, q, part), opiece(d, q, part), os_.at[0], zc.at[d - 1], sp=mate).wait_recv()

    def by_side(work):
        for side in range(2):
            for core in range(2):
                @pl.when((odd == side) & (t == core))
                def _(side=side, core=core):
                    work(side, core)

    def relay_out(d, to_d):
        q = order(d, 0)
        return remote(opiece(d, q), opiece(3, q), os_.at[0], or_.at[2, q], fs=f ^ to_d)

    def assist(i):
        q = 2 * odd + i
        return remote(opiece(3, q), opiece(3, q), os_.at[0], or_.at[2, q], sp=mate)

    row_arrived(1, 0)
    row_send(1, 0, 2).start()
    row_arrived(2, 1)
    row_send(2, 1, 1).start()
    pltpu.make_async_copy(wo.at[0], wo.at[0], oloc.at[0]).wait()
    for i in range(2):
        own_out(1, i).start()
        own_out(2, i).start()

    zhop(1, 2)
    zhop(2, 1)
    zhop(2, 2)
    send_own(3, inner)
    row_arrived(1, 1)
    twin(1).start()
    row_arrived(2, 0)
    twin(2).start()
    zhop(1, 3)
    send_own(4, inner)

    def project(d, n, p, q):
        left = rows[pl.ds(d, n)].reshape(n * length, rows.shape[2])
        co = pl.ds(p * wide, (q - p) * wide)
        made = jnp.dot(left, wg[:, co], preferred_element_type=F32).astype(BF)
        y[pl.ds(d, n), :, co] = made.reshape(n, length, (q - p) * wide)

    def group(d, p):
        return y[d, :, p * wide : (p + 1) * wide]

    causal = ri >= ci
    tril_short = tril.astype(BF)

    def local(d):
        fl = floor[f]
        logits = group(d, FORGET).astype(F32)
        retain = fl + (1.0 - fl) * jax.nn.sigmoid(logits)
        keys = (1.0 - fl) * jax.nn.sigmoid(-logits)
        step = jnp.log(retain)
        coarse = step.astype(BF)
        fine = (step - coarse.astype(F32)).astype(BF)
        both = jnp.dot(
            tril_short, jnp.concatenate([coarse, fine], axis=1), preferred_element_type=F32
        )
        total = both[:, :wide] + both[:, wide:]
        raw = group(d, QUERY).astype(F32)
        query = raw * jax.nn.sigmoid(raw) * jnp.exp(total)
        value = group(d, VALUE)
        scores = lax.dot_general(
            query.astype(BF), (keys * jnp.exp(-total)).astype(BF), NT, preferred_element_type=F32
        )
        lc = lcol[d]
        gap = lc[:, 0:1] - lrow[d, 0:1, :]
        scores = jnp.where(causal, scores * jnp.exp(jnp.where(causal, gap, 0.0)), 0.0)
        inside[d] = jnp.dot(scores.astype(BF), value, preferred_element_type=F32)
        reach[d] = (query * jnp.exp(lc)).astype(BF)
        full = total + lc
        end = full[length - 1 :, :]
        update = (keys * jnp.exp(end - full)).astype(BF)
        states[d] = lax.dot_general(value, update, TN, preferred_element_type=F32)
        sdecay[d] = jnp.broadcast_to(jnp.exp(end), (8, wide))

    def many(body, first, last):
        def one(d, carry):
            body(d)
            return carry

        lax.fori_loop(first, last, one, 0)

    for load in loads[4:]:
        load.wait()
    twin_arrived(0)
    zready(0)
    zready(1)
    project(0, 1, 0, 2)
    twin_arrived(1)
    twin_arrived(2)
    project(1, 2, 0, 2)
    zready(2)
    project(0, 1, 2, 3)
    project(1, 2, 2, 3)
    row_arrived(3, 0)
    row_arrived(3, 1)
    twin(3).start()
    many(local, 0, 3)
    zhop(2, 3)
    zhop(1, 4)
    zhop(2, 4)
    twin_arrived(3)
    project(3, 1, 0, 2)
    project(3, 1, 2, 3)
    many(local, 3, 4)

    out_arrived(2, order(2, 0))
    relay_out(2, 1).start()
    out_arrived(1, order(1, 0))
    relay_out(1, 2).start()

    def state_copy(d):
        return remote(sout.at[d], sin.at[d], ss.at[0], sr.at[d], sp=s + 1)

    def place(j, g):
        return mix.at[:, pl.ds(pl.multiple_of(j * depth + g * wide, wide), wide)]

    def mixed_send(d, j):
        return remote(msend.at[d - 1, j], place(j, f), xs.at[0], xr.at[0], fs=f ^ d)

    def deliver(d, j, value):
        if d == 0:
            mix[:, pl.ds(pl.multiple_of(j * depth + f * wide, wide), wide)] = value
        else:
            msend[d - 1, j] = value
            mixed_send(d, j).start()

    def chain(d):
        @pl.when(has_left)
        def _():
            state_copy(d).wait_recv()

        @pl.when(s == 0)
        def _():
            sin[d] = jnp.zeros(sin.shape[1:], BF)

        @pl.when(has_right)
        def _():
            sout[d] = (sin[d].astype(F32) * sdecay[d, 0:1, :] + states[d]).astype(BF)
            state_copy(d).start()

        raw = inside[d] + lax.dot_general(reach[d], sin[d], NT, preferred_element_type=F32)
        scale = lax.rsqrt(jnp.mean(raw * raw, axis=-1, keepdims=True) + 1e-06)
        deliver(d, 1, (raw * scale * hgain[...]).astype(BF))

    turns = (3, 1, 2, 0)
    last = s == ns - 1
    inland = jnp.logical_not(last)


    edge = rim.shape[1]

    def rim_copy():
        return remote(brim, rim, ms.at[0], mr.at[0], sp=s + 1)

    def swaps(side):
        for core in range(2):
            @pl.when(t == core)
            def _(core=core):
                for d in (1, 2):
                    swap(d, side, core).start()

    def signal():
        zready(3)

        @pl.when(has_right)
        def _():
            ends_ = rows[:, pl.ds(length - edge, edge), :].reshape(nf * edge, rows.shape[2])
            made = jnp.dot(ends_, wg[:, pl.ds(SIGNAL * wide, wide)], preferred_element_type=F32).astype(BF)
            brim[...] = made.reshape(nf, edge, wide)
            rim_copy().start()

        @pl.when(s == 0)
        def _():
            rim[...] = jnp.zeros(rim.shape, BF)

        @pl.when((odd == 0) & (s > 0))
        def _():
            swaps(0)

        def one(d, carry):
            project(d, 1, 3, 4)
            return carry

        lax.fori_loop(0, nf, one, 0)

    def assists():
        for i in range(2):
            out_arrived(3, 2 * odd + i)
            assist(i).start()

    @pl.when(odd == 1)
    def _():
        swaps(1)

    def thirds():
        for to_d in (1, 2):
            third_upper(to_d).start()

    @pl.when(last)
    def _():
        thirds()
        signal()
        assists()

    for d in turns:
        chain(d)

    @pl.when(s == 0)
    def _():
        swaps(0)

    @pl.when(inland)
    def _():
        thirds()
        signal()

    @pl.when(inland)
    def _():
        assists()


    @pl.when(has_left)
    def _():
        rim_copy().wait_recv()

    def filtering(d):
        padded = jnp.concatenate([rim[d], group(d, SIGNAL)], axis=0).astype(F32)
        margin = taps.shape[1] - 1
        filtered = jnp.zeros((length, wide), F32)
        for o in range(margin + 1):
            start = edge - margin + o
            filtered = filtered + taps[f, o : o + 1, :] * padded[start : start + length]
        filt[d] = filtered

    many(filtering, 0, nf)
    zready(4)
    for d in turns:
        project(d, 1, 4, 5)
        deliver(d, 0, (group(d, GATE).astype(F32) * filt[d]).astype(BF))
    for to_d in (1, 2):
        third_lower(to_d).start()

    def fourths(side, core):
        for to_d in (1, 2):
            fourth(to_d, side, core).start()

    by_side(fourths)


    mixed = remote(msend, msend, xs.at[0], xr.at[0], fs=f ^ 1)
    mixed.wait_recv()

    def rows_of(core):
        return pl.ds(pl.multiple_of(core * half, half), half)

    def finish(chunks):
        spans = []
        for d, c in chunks:
            co = pl.ds(pl.multiple_of(c * 2 * pw, 2 * pw), 2 * pw)
            at = pl.ds(pl.multiple_of((f ^ d) * cols + c * 2 * pw, 2 * pw), 2 * pw)
            shares[:, at] = jnp.dot(mix[...], wo[d, :, co], preferred_element_type=F32).astype(BF)
            spans.append(at)
        for at in spans:
            remote(shares.at[rows_of(other), at], twin_part.at[0, :, at], es.at[0], er.at[0], tp=other).start()
        for at in spans:
            pltpu.make_async_copy(shares.at[rows_of(t), at], part.at[0, :, at], fin.at[0]).start()

    def last_quarters(d):
        third_upper(d).wait_recv()
        out_arrived(d, order(d, 2), lower)

        def rest(side, core):
            swapped(d, side, core)
            out_arrived(d, order(d, 3), (taken(side, core), 2 * depth - taken(side, core)))

        by_side(rest)

    def assisted(d):
        for q in (2 - 2 * odd, 3 - 2 * odd):
            out_arrived(3, q)

    for d in (1, 2):
        out_arrived(d, order(d, 1))
    finish([(0, odd), (0, 1 - odd), (1, odd), (2, odd), (3, odd)])
    for d in (1, 2):
        last_quarters(d)
    assisted(3)
    finish([(1, 1 - odd), (2, 1 - odd), (3, 1 - odd)])


    def drained(ref, sem):
        pltpu.make_async_copy(ref, ref, sem).wait()

    @pl.when(inner)
    def _():
        drained(wg, zs.at[0])

    own_rows = wg.at[pl.ds(pl.multiple_of(s * kd, kd), kd), :]

    @pl.when(s == 0)
    def _():
        drained(own_rows, zs.at[0])

    @pl.when(has_left)
    def _():
        drained(own_rows, zsl.at[0])

    drained(rows.at[pl.ds(0, 3), pl.ds(0, half), :], rs.at[0])
    drained(rows.at[:, pl.ds(0, half), :], ts.at[0])
    drained(others, ls.at[0])
    drained(msend, xs.at[0])

    def quarters(side, core):
        count = 2 * (8 * depth - taken(side, core)) + 8 * depth + 2 * taken(1 - side, core)
        drained(wo.at[:, pl.ds(0, count // 16), :], os_.at[0])

    by_side(quarters)

    @pl.when(has_right)
    def _():
        drained(sout, ss.at[0])
        drained(brim, ms.at[0])

    mine = shares.at[rows_of(t), :]
    drained(mine, es.at[0])
    drained(mine, fin.at[0])
    drained(mine, er.at[0])


def body(ns, nf, tokens, norm_gain, w0, w1, w2, w3, w4, conv_taps, floor_gate, leak, head_gain, cow, how):
    half, width = tokens.shape[1:]
    length = 2 * half
    heads = leak.shape[2]
    kd = w0.shape[0]
    wide = w0.shape[1] // nf
    assert heads == nf and nf == 4 and floor_gate.shape[0] == heads * wide and ns % 2 == 0
    taps = conv_taps.reshape(conv_taps.shape[0], nf, wide).transpose(1, 0, 2)
    hbm = pl.BlockSpec(memory_space=pltpu.HBM)
    dma = pltpu.SemaphoreType.DMA
    depth, cols = cow.shape
    scratch = [
        pltpu.VMEM((half, width), BF),
        pltpu.VMEM((1, width), F32),
        pltpu.VMEM(taps.shape, F32),
        pltpu.VMEM((heads, 1, wide), F32),
        pltpu.VMEM((heads, length), F32),
        pltpu.VMEM((1, wide), F32),
        pltpu.VMEM((nf, length, width), BF),
        pltpu.VMEM((ns * kd, 5 * wide), BF),
        pltpu.VMEM((nf, length, 5 * wide), BF),
        pltpu.VMEM((nf, 2 * depth, cols), BF),
        pltpu.VMEM((nf, 16, wide), BF),
        pltpu.VMEM((nf, 16, wide), BF),
        pltpu.VMEM((nf, length, wide), F32),
        pltpu.VMEM((nf, length, wide), F32),
        pltpu.VMEM((nf, length, wide), BF),
        pltpu.VMEM((nf, wide, wide), F32),
        pltpu.VMEM((nf, 8, wide), F32),
        pltpu.VMEM((nf, wide, wide), BF),
        pltpu.VMEM((nf, wide, wide), BF),
        pltpu.VMEM((nf, 8, length), F32),
        pltpu.VMEM((nf, length, wide), F32),
        pltpu.VMEM((nf, 8, length), F32),
        pltpu.VMEM((nf - 1, 2, length, wide), BF),
        pltpu.VMEM((length, 2 * depth), BF),
        pltpu.VMEM((length, width), BF),
        dma((7,)), dma((1,)), dma((1,)), dma((ns, 5)), dma((5,)),
        dma((1,)), dma((nf - 1, 2)), dma((1,)), dma((nf,)), dma((1,)), dma((1,)),
        dma((1,)), dma((1,)), dma((3, 4)), dma((2,)), dma((2,)),
        dma((1,)), dma((1,)), dma((1,)), dma((1,)), dma((1,)), dma((nf,)),
        dma((1,)), dma((1,)), dma((1,)),
    ]
    part, twin_part = pl.pallas_call(
        functools.partial(kernel, ns, nf),
        out_shape=[jax.ShapeDtypeStruct(tokens.shape, BF)] * 2,
        in_specs=[hbm] * 13,
        out_specs=[hbm] * 2,
        scratch_shapes=scratch,
        compiler_params=pltpu.CompilerParams(
            collective_id=0, has_side_effects=True, vmem_limit_bytes=60 * 2**20
        ),
    )(
        tokens, norm_gain[None], w0, w1, w2, w3, w4, taps, floor_gate.reshape(heads, 1, wide),
        leak[0].T, head_gain[None], cow, how,
    )
    return (part.astype(F32) + twin_part.astype(F32)).astype(BF)


def solution(mesh):
    in_specs = (
        P("fs", ("sp", "tp"), None),
        P(),
        P("sp", "tp"),
        P("sp", "tp"),
        P("sp", "tp"),
        P("sp", "tp"),
        P("sp", "tp"),
        P(None, "tp"),
        P("tp"),
        P("fs", "sp", "tp"),
        P(),
        P("tp", "fs"),
        P("tp", "fs"),
    )
    out_specs = P("fs", ("sp", "tp"), None)
    step = functools.partial(body, mesh.shape["sp"], mesh.shape["fs"])
    return jax.shard_map(step, mesh=mesh, in_specs=in_specs, out_specs=out_specs, check_vma=False)
```
